512 devices in a mesh: sp: 32 (over z, x), tp: 16 (over y, core).
Axes of the slice: x: 4, y: 8, z: 8, core: 2. Of those that a mesh axis runs over, the one named last changes fastest.
Arguments:
- cotangent: bfloat16 [4096, 2048], P('sp'), may hold values from -6 to 6
- stream: bfloat16 [4096, 2048], P('sp'), may hold values from -6 to 6
- routes: int32 [4096, 2], P('sp'), may hold values from 0 to 15, all different within a row; in each aligned block of 128 rows (0 to 127, 128 to 255, ...) at most 24 rows name the same one
- route_weights: float32 [4096, 2], P('sp'), may hold values from 0.25 to 1
- gate_weight: bfloat16 [32, 2048, 2048], P('sp', None, 'tp'), may hold values from -0.125 to 0.125
- up_weight: bfloat16 [32, 2048, 2048], P('sp', None, 'tp'), may hold values from -0.125 to 0.125
- down_weight: bfloat16 [32, 2048, 2048], P('sp', 'tp'), may hold values from -0.09375 to 0.09375
- outer_gate: bfloat16 [4096, 1024], P('sp', 'tp'), may hold values from -6 to 6
- inner_gate: bfloat16 [4096, 1024], P('sp', 'tp'), may hold values from -6 to 6
- conv_input: bfloat16 [4096, 1024], P('sp', 'tp'), may hold values from -6 to 6
- conv_taps: bfloat16 [3, 1024], P(None, 'tp'), may hold values from -1 to 1
- out_weight: bfloat16 [2048, 1024], P(None, 'tp'), may hold values from -0.1875 to 0.1875
Outputs:
- gate_grad: bfloat16 [32, 2048, 2048], P('sp', None, 'tp')
- up_grad: bfloat16 [32, 2048, 2048], P('sp', None, 'tp')
- down_grad: bfloat16 [32, 2048, 2048], P('sp', 'tp')
- out_grad: float32 [2048, 1024], P('sp', 'tp')
- outer_grad: bfloat16 [4096, 1024], P('sp', 'tp')
- inner_grad: bfloat16 [4096, 1024], P('sp', 'tp')
- input_grad: bfloat16 [4096, 1024], P('sp', 'tp')
The draws below stay inside these ranges and needn't reach their ends.
Inputs may be any that keep to these rules, and one draw needn't show every extreme that they name: `routes`: each token names two different experts. Among the 128 tokens of one index of sp no expert is named by more than 24 tokens, a bound that some block of them reaches in every draw.
All inputs are finite; a program needn't handle non-finite values.
Results may differ from the reference program's by a relative error of at most 0.02.
Values may be sent and summed in bfloat16 or wider, within the bound.
No kernel may reach another device: no remote copies, remote signals or barrier semaphores. Data moves between devices by JAX's collectives and lax.ppermute only.
A program may use at most 64 MiB of HBM per device.

```python
import math
import jax
import jax.numpy as jnp
import numpy as np
from jax import lax

D = 2048
HID = 4096
CONV = 1024
TOK_DEV = 128
HALF = 2048
CAP = 24
TOKENS = 4096
N_SP = 32
N_TP = 16


def with_spikes(entries, own_key, source, target, shards_of, factor):
    def block_of(axis_at):
        return (jnp.arange(entries.shape[axis_at]) // (entries.shape[axis_at] // shards_of)).reshape((-1,) + (1,) * (entries.ndim - 1 - axis_at))

    near = jax.random.permutation(own_key, shards_of)[block_of(target)]
    far = (block_of(target) + shards_of // 2) % shards_of
    return jnp.where((block_of(source) == near) | (block_of(source) == far), factor * entries, entries)


def block_levels(key, extent, cuts, smallest, largest):
    def one(position, parts):
        steps = jax.random.uniform(jax.random.fold_in(jax.random.fold_in(key, 6), position), (parts,), jnp.float32, smallest / len(cuts), largest / len(cuts))
        return jnp.repeat(jnp.exp(steps), extent[position] // parts).reshape((-1,) + (1,) * (len(extent) - position - 1))

    loudness = one(*cuts[0])
    for cut in cuts[1:]:
        loudness = loudness * one(*cut)
    return loudness


def routed_block(key, own, number, rows, number_of, top, most, skew):
    ranking = jax.random.permutation(key, number_of)
    crowded, ordinary = portions_of(number_of, rows * top, most, skew, True), portions_of(number_of, rows * top, most, skew, False)
    places = jnp.arange(number_of)

    def named(sizes, rotation):
        used = int((sizes > 0).sum())
        fixed = max(1, used // 4)
        shifted = fixed + (places - fixed + rotation * (used - fixed)) % max(1, number_of - fixed)
        return jnp.zeros((number_of,), jnp.int32).at[ranking[jnp.where(places < fixed, places, shifted)]].set(jnp.asarray(sizes, jnp.int32))

    sizes = jnp.where(number % 4 == 0, named(crowded, number // 4), named(ordinary, number - number // 4 - 1))
    mixed = jax.random.permutation(jax.random.fold_in(own, 3), number_of)
    donor, sink = mixed[0:number_of // 2 * 2:2], mixed[1:number_of // 2 * 2:2]
    margin = jnp.minimum(sizes[donor] - 1, most - sizes[sink]) // 2
    margin = jnp.where((donor == ranking[0]) | (sink == ranking[0]) | (sizes[sink] == 0), 0, jnp.maximum(margin, 0))
    shifted = jax.random.randint(jax.random.fold_in(own, 4), (number_of // 2,), 0, 1 << 20) % (margin + 1)
    sizes = sizes.at[donor].add(-shifted).at[sink].add(shifted)
    items = jnp.searchsorted(jnp.cumsum(sizes), jnp.arange(rows * top), side="right").astype(jnp.int32)
    grid = items.reshape(top, rows).T
    grid = grid[jax.random.permutation(jax.random.fold_in(own, 1), rows)]
    rotation = jax.random.randint(jax.random.fold_in(own, 2), (rows, 1), 0, top)
    return jnp.take_along_axis(grid, (jnp.arange(top)[None, :] + rotation) % top, axis=1)


def portions_of(count, total, reach, skew, full):
    weights = [(1 << 20) // math.isqrt(rank ** skew) + 1 for rank in range(1, count + 1)]
    largest = reach if full else min(reach, max(-(-total // count), total * weights[0] // sum(weights)))
    least = 1 if total - largest >= count - 1 else 0
    given, rest = [largest] + [least] * (count - 1), total - largest - least * (count - 1)
    while rest > 0:
        movable = [i for i in range(1, count) if given[i] < largest] or [i for i in range(1, count) if given[i] < reach]
        mass, left = sum([weights[i] for i in movable]), rest
        for i in movable:
            extra = min(reach - given[i], max(1, left * weights[i] // mass), rest)
            given[i] = given[i] + extra
            rest = rest - extra
    return np.array(given)


def scatter_about(stream_key, extent, spread, most, cuts=(), held_as=jnp.bfloat16):
    result = spread * jax.random.normal(stream_key, extent, jnp.float32)
    if cuts:
        result = result * block_levels(stream_key, extent, cuts, -0.22, 0.18)
    return jnp.clip(result, -most, most).astype(held_as)


def gaussian_with(key, shape, scale, most, pieces, heavy, kind=jnp.bfloat16):
    array = scale * jax.random.normal(key, shape, jnp.float32)
    if pieces:
        array = array * block_levels(key, shape, pieces, -0.22, 0.18)
    return jnp.clip(with_spikes(array, jax.random.fold_in(key, 3), *heavy), -most, most).astype(kind)


def setup_inputs(seed: int = 0) -> dict:
    keys = jax.random.split(jax.random.key(seed), 13)
    cotangent = gaussian_with(keys[0], (TOKENS, D), 1.0, 6.0, ((0, 32),), (0, 1, 32, 2.75))
    stream = scatter_about(keys[1], (TOKENS, D), 1.0, 6.0, ((0, 32),))
    routes_keys = jax.random.split(jax.random.fold_in(keys[2], 1), TOKENS // TOK_DEV)
    routes_turns = jax.random.permutation(jax.random.fold_in(keys[2], 3), TOKENS // TOK_DEV)
    routes = jax.vmap(lambda own, number: routed_block(jax.random.fold_in(keys[2], 2), own, number, TOK_DEV, N_SP // 2, 2, CAP, 1))(routes_keys, routes_turns).reshape((TOKENS, 2))
    route_weights = jnp.clip(0.25 + 0.75 * jax.random.uniform(keys[3], (TOKENS, 2), jnp.float32) ** block_levels(keys[3], (TOKENS, 2), ((0, 32),), -0.2, 0.2), 0.25, 1.0)
    gate_weight = scatter_about(keys[4], (N_SP, D, HALF), D ** -0.5, 0.125, ((0, 32), (2, 16)))
    up_weight = scatter_about(keys[5], (N_SP, D, HALF), D ** -0.5, 0.125, ((0, 32), (2, 16)))
    down_weight = scatter_about(keys[6], (N_SP, HALF, D), HID ** -0.5, 0.09375, ((0, 32), (1, 16)))
    outer_gate = scatter_about(keys[7], (TOKENS, CONV), 1.0, 6.0, ((0, 32), (1, 16)))
    inner_gate = scatter_about(keys[8], (TOKENS, CONV), 1.0, 6.0, ((0, 32), (1, 16)))
    conv_input = scatter_about(keys[9], (TOKENS, CONV), 1.0, 6.0, ((0, 32), (1, 16)))
    conv_taps = jnp.clip(jax.random.uniform(keys[10], (3, CONV), jnp.float32, -1.0, 1.0) * block_levels(keys[10], (3, CONV), ((1, 16),), -0.4, 0.0), -1.0, 1.0).astype(jnp.bfloat16)
    out_weight = scatter_about(keys[11], (D, CONV), CONV ** -0.5, 0.1875, ((1, 16),))
    return {"cotangent": cotangent, "stream": stream, "routes": routes, "route_weights": route_weights, "gate_weight": gate_weight, "up_weight": up_weight, "down_weight": down_weight, "outer_gate": outer_gate, "inner_gate": inner_gate, "conv_input": conv_input, "conv_taps": conv_taps, "out_weight": out_weight}


def reference(cotangent, stream, routes, route_weights, gate_weight, up_weight, down_weight, outer_gate, inner_gate, conv_input, conv_taps, out_weight):
    tok_count = stream.shape[0]
    model_width = stream.shape[1]
    experts = N_SP // 2
    limit = N_SP * CAP
    blocks = N_TP
    block_units = HALF // N_TP
    flat_routes = routes.reshape(-1).astype(jnp.int32)
    flat_weights = route_weights.reshape(-1).astype(jnp.float32)
    flat_tokens = (jnp.arange(2 * tok_count) // 2).astype(jnp.int32)

    def one_expert(moe_sum, index):
        hits = flat_routes == index
        picked = jnp.nonzero(hits, size=limit, fill_value=0)[0].astype(jnp.int32)
        live_mask = jnp.arange(limit) < jnp.sum(hits.astype(jnp.int32))
        tok_index = flat_tokens[picked]
        weights = jnp.where(live_mask, flat_weights[picked], jnp.float32(0.0))
        routed_rows = jnp.where(live_mask[:, None], stream[tok_index], jnp.zeros((), jnp.bfloat16))
        routed_cot = (weights[:, None] * cotangent[tok_index].astype(jnp.float32)).astype(jnp.bfloat16)
        gate_pair = lax.dynamic_slice_in_dim(gate_weight, 2 * index, 2, 0)
        up_pair = lax.dynamic_slice_in_dim(up_weight, 2 * index, 2, 0)
        down_pair = lax.dynamic_slice_in_dim(down_weight, 2 * index, 2, 0)
        gate_full = jnp.concatenate([gate_pair[0], gate_pair[1]], axis=1)
        up_full = jnp.concatenate([up_pair[0], up_pair[1]], axis=1)
        down_full = jnp.concatenate([down_pair[0], down_pair[1]], axis=0)
        gate_pre = jnp.dot(routed_rows, gate_full, preferred_element_type=jnp.float32)
        up_pre = jnp.dot(routed_rows, up_full, preferred_element_type=jnp.float32)
        hidden_grad = jnp.dot(routed_cot, down_full.T, preferred_element_type=jnp.float32)
        sigma = jax.nn.sigmoid(gate_pre)
        silu_gate = gate_pre * sigma
        hidden = (silu_gate * up_pre).astype(jnp.bfloat16)
        up_delta = (hidden_grad * silu_gate).astype(jnp.bfloat16)
        gate_delta = (hidden_grad * up_pre * sigma * (1.0 + gate_pre * (1.0 - sigma))).astype(jnp.bfloat16)
        gate_grad = jnp.dot(routed_rows.T, gate_delta, preferred_element_type=jnp.float32).astype(jnp.bfloat16)
        up_grad = jnp.dot(routed_rows.T, up_delta, preferred_element_type=jnp.float32).astype(jnp.bfloat16)
        down_grad = jnp.dot(hidden.T, routed_cot, preferred_element_type=jnp.float32).astype(jnp.bfloat16)
        gate_blocks = gate_delta.astype(jnp.float32).reshape(limit, 2 * blocks, block_units)
        up_blocks = up_delta.astype(jnp.float32).reshape(limit, 2 * blocks, block_units)
        gate_table = gate_full.astype(jnp.float32).reshape(model_width, 2 * blocks, block_units)
        up_table = up_full.astype(jnp.float32).reshape(model_width, 2 * blocks, block_units)
        block_part = jnp.einsum("sgh,dgh->gsd", gate_blocks, gate_table) + jnp.einsum("sgh,dgh->gsd", up_blocks, up_table)
        block_part = lax.optimization_barrier(block_part.astype(jnp.bfloat16)).astype(jnp.float32)
        half_sums = jnp.sum(block_part.reshape(2, blocks, limit, model_width), axis=1)
        half_sums = lax.optimization_barrier(half_sums.astype(jnp.bfloat16)).astype(jnp.float32)
        route_sum = jnp.where(live_mask[:, None], half_sums[0] + half_sums[1], jnp.float32(0.0))
        moe_sum = moe_sum.at[tok_index].add(route_sum)
        gate_out = jnp.transpose(gate_grad.reshape(model_width, 2, HALF), (1, 0, 2))
        up_out = jnp.transpose(up_grad.reshape(model_width, 2, HALF), (1, 0, 2))
        down_out = down_grad.reshape(2, HALF, model_width)
        return moe_sum, (gate_out, up_out, down_out)

    moe_sum, stacked = lax.scan(one_expert, jnp.zeros((tok_count, model_width), jnp.float32), jnp.arange(experts, dtype=jnp.int32))
    gate_grad = stacked[0].reshape(N_SP, model_width, HALF)
    up_grad = stacked[1].reshape(N_SP, model_width, HALF)
    down_grad = stacked[2].reshape(N_SP, HALF, model_width)
    moe_grad = moe_sum.astype(jnp.bfloat16)
    stream_grad = (cotangent.astype(jnp.float32) + moe_grad.astype(jnp.float32)).astype(jnp.bfloat16)

    taps = conv_taps.astype(jnp.float32)
    mixed = inner_gate.astype(jnp.float32) * conv_input.astype(jnp.float32)
    padded = jnp.pad(mixed, ((2, 0), (0, 0)))
    conv_sum = taps[0] * padded[:-2] + taps[1] * padded[1:-1] + taps[2] * padded[2:]
    conv_out = (outer_gate.astype(jnp.float32) * conv_sum).astype(jnp.bfloat16)
    out_grad = jnp.dot(stream_grad.T, conv_out, preferred_element_type=jnp.float32)
    conv_grad = jnp.dot(stream_grad, out_weight, preferred_element_type=jnp.float32)
    outer_grad = (conv_grad * conv_sum).astype(jnp.bfloat16)
    scaled = conv_grad * outer_gate.astype(jnp.float32)
    later = jnp.pad(scaled, ((0, 2), (0, 0)))
    mixed_grad = taps[2] * later[:-2] + taps[1] * later[1:-1] + taps[0] * later[2:]
    inner_grad = (mixed_grad * conv_input.astype(jnp.float32)).astype(jnp.bfloat16)
    input_grad = (mixed_grad * inner_gate.astype(jnp.float32)).astype(jnp.bfloat16)
    return (gate_grad, up_grad, down_grad, out_grad, outer_grad, inner_grad, input_grad)
```

```python
import functools

import jax
import jax.numpy as jnp
from jax import lax
from jax.experimental import pallas as pl
from jax.experimental.pallas import tpu as pltpu
from jax.sharding import Mesh, PartitionSpec as P

BF16, F32, I32 = jnp.bfloat16, jnp.float32, jnp.int32
TP = ("y", "c")
NT = (((1,), (1,)), ((), ()))
TN = (((0,), (0,)), ((), ()))
LANES = 128
VMEM = pl.BlockSpec(memory_space=pltpu.VMEM)


def mm(a, b, dims=None):
    if dims is None:
        return jnp.dot(a, b, preferred_element_type=F32)
    return lax.dot_general(a, b, dims, preferred_element_type=F32)


def call(body, out, cost, **kw):
    flops, moved = cost
    return pl.pallas_call(
        body,
        out_shape=out,
        cost_estimate=pl.CostEstimate(flops=flops, bytes_accessed=moved, transcendentals=0),
        compiler_params=pltpu.CompilerParams(vmem_limit_bytes=48 * 1024 * 1024),
        **kw,
    )


def shape(dims, kind):
    return jax.ShapeDtypeStruct(dims, kind)


def select_body(experts, capacity, at_ref, routes_ref, weights_ref, rows_ref, cot_ref, send_ref, select_ref):
    tokens = routes_ref.shape[1]
    number = lax.broadcasted_iota(I32, (experts, tokens), 0)
    first = routes_ref[0:1, :] == number
    second = routes_ref[1:2, :] == number
    hit = jnp.where(first | second, 1.0, 0.0).astype(F32)
    weight = jnp.where(first, weights_ref[0:1, :], jnp.where(second, weights_ref[1:2, :], 0.0))
    earlier = lax.broadcasted_iota(I32, (tokens, tokens), 0) < lax.broadcasted_iota(I32, (tokens, tokens), 1)
    place = mm(hit.astype(BF16), jnp.where(earlier, 1.0, 0.0).astype(BF16))
    place = jnp.where(hit > 0.0, place, -1.0)
    slot = lax.broadcasted_iota(I32, (capacity, tokens), 0).astype(F32)
    picked, scales = [], []
    for e in range(experts):
        one = jnp.where(slot == place[e : e + 1, :], 1.0, 0.0)
        scale = jnp.sum(one * weight[e : e + 1, :], axis=1, keepdims=True)
        picked += [one, one]
        scales += [scale, scale]
    select = jnp.concatenate(picked, axis=0).astype(BF16)
    scale = jnp.concatenate(scales, axis=0)
    select_ref[...] = select
    send_ref[:, :LANES] = mm(select, rows_ref[...]).astype(BF16)
    send_ref[:, LANES:] = (mm(select, cot_ref[...]) * scale).astype(BF16)


def expert_body(steps, core_ref, got_ref, gate_ref, up_ref, down_ref, delta_ref, hidden_ref, own_ref, other_ref, both):
    @pl.when(pl.program_id(0) == 0)
    def _():
        both[:, :LANES] = gate_ref[...]
        both[:, LANES:] = up_ref[...]

    rows = got_ref.shape[1]
    pre = jnp.zeros((rows, 2 * LANES), F32)
    back = jnp.zeros((rows, LANES), F32)
    for k in range(steps):
        ch = slice(k * 2 * LANES, (k + 1) * 2 * LANES)
        x = jnp.concatenate([got_ref[2 * k, :, :LANES], got_ref[2 * k + 1, :, :LANES]], axis=1)
        d = jnp.concatenate([got_ref[2 * k, :, LANES:], got_ref[2 * k + 1, :, LANES:]], axis=1)
        pre = pre + mm(x, both[ch, :])
        back = back + mm(d, down_ref[:, ch], NT)
    gate, up = pre[:, :LANES], pre[:, LANES:]
    sigma = jax.nn.sigmoid(gate)
    silu = gate * sigma
    hidden_ref[...] = (silu * up).astype(BF16)
    delta = jnp.concatenate(
        [
            (back * up * sigma * (1.0 + gate * (1.0 - sigma))).astype(BF16),
            (back * silu).astype(BF16),
        ],
        axis=1,
    )
    delta_ref[...] = delta
    core = core_ref[0]
    for y in range(0, steps, 2):
        for ref, c in ((other_ref, 1 - core), (own_ref, core)):
            lo = both[pl.ds(pl.multiple_of((2 * y + c) * LANES, LANES), LANES), :]
            hi = both[pl.ds(pl.multiple_of((2 * y + 2 + c) * LANES, LANES), LANES), :]
            part = mm(delta, jnp.concatenate([lo, hi], axis=0), NT).astype(BF16)
            ref[y] = part[:, :LANES]
            ref[y + 1] = part[:, LANES:]


def weight_body(got_ref, delta_ref, hidden_ref, gate_ref, up_ref, down_ref):
    x = jnp.concatenate([got_ref[0, :, :LANES], got_ref[1, :, :LANES]], axis=1)
    d = jnp.concatenate([got_ref[0, :, LANES:], got_ref[1, :, LANES:]], axis=1)
    grads = mm(x, delta_ref[...], TN)
    gate_ref[...] = grads[:, :LANES].astype(BF16)
    up_ref[...] = grads[:, LANES:].astype(BF16)
    down_ref[...] = mm(hidden_ref[...], d, TN).astype(BF16)


def token_body(at_ref, back_ref, select_ref, cot_ref, conv_ref, grad_ref, out_ref):
    moe = mm(select_ref[...], back_ref[...], TN).astype(BF16)
    grad = (cot_ref[...].astype(F32) + moe.astype(F32)).astype(BF16)
    grad_ref[...] = grad
    flipped = grad.astype(F32).T.astype(BF16)
    count, width, tokens = conv_ref.shape
    half = width // 2
    left = jnp.concatenate([flipped[r * width : r * width + half] for r in range(2)], axis=0)
    right = jnp.concatenate([flipped[r * width + half : (r + 1) * width] for r in range(2)], axis=0)
    lhs = jnp.concatenate([left, right], axis=1)
    blank = jnp.zeros((width, tokens), BF16)
    for j in range(0, count, 2):
        rhs = []
        for k in (j, j + 1):
            rhs += [jnp.concatenate([conv_ref[k], blank], axis=1), jnp.concatenate([blank, conv_ref[k]], axis=1)]
        part = mm(lhs, jnp.concatenate(rhs, axis=0), NT).astype(BF16)
        for r in range(2):
            rows = part[r * half : (r + 1) * half]
            out_ref[r * count + j] = rows[:, :LANES]
            out_ref[r * count + j + 1] = rows[:, LANES:]


def conv_body(steps, grads_ref, weight_ref, sum_ref, outer_ref, outer_grad_ref, scaled_ref):
    total = jnp.zeros(sum_ref.shape, F32)
    for k in range(steps):
        g = jnp.concatenate([grads_ref[2 * k], grads_ref[2 * k + 1]], axis=1)
        total = total + mm(weight_ref[:, k * 2 * LANES : (k + 1) * 2 * LANES], g, NT)
    outer_grad_ref[...] = (total * sum_ref[...]).astype(BF16)
    scaled_ref[...] = total * outer_ref[...].astype(F32)


def per_device(
    cotangent,
    stream,
    routes,
    route_weights,
    gate_weight,
    up_weight,
    down_weight,
    outer_gate,
    inner_gate,
    conv_input,
    conv_taps,
    out_weight,
):
    groups = lax.axis_size("sp")
    ys = lax.axis_size("y")
    tps = 2 * ys
    experts = groups // 2
    tokens, width = stream.shape
    capacity = 3 * tokens // experts
    slots = groups * capacity
    units = gate_weight.shape[2]
    channels = outer_gate.shape[1]
    core = lax.axis_index("c").astype(I32).reshape(1)
    at = (2 * lax.axis_index("y") + lax.axis_index("c")).astype(I32).reshape(1)
    swap = [(0, 1), (1, 0)]

    block = pl.BlockSpec((tokens, LANES), lambda i, at: (0, at[0]))
    whole = lambda *dims: pl.BlockSpec(dims, lambda i, at: (0,) * len(dims))
    send, select = call(
        functools.partial(select_body, experts, capacity),
        (shape((slots, 2 * LANES), BF16), shape((slots, LANES), BF16)),
        (2 * slots * tokens * 2 * LANES, 2**20),
        grid_spec=pltpu.PrefetchScalarGridSpec(
            num_scalar_prefetch=1,
            grid=(1,),
            in_specs=[whole(2, tokens), whole(2, tokens), block, block],
            out_specs=[whole(slots, 2 * LANES), whole(slots, LANES)],
        ),
    )(at, routes.T, route_weights.T, stream, cotangent)
    recv = lax.all_to_all(
        send.reshape(groups, capacity, 2 * LANES), "sp", split_axis=0, concat_axis=0, tiled=True
    ).reshape(slots, 2 * LANES)

    outer_t, inner_t, input_t, taps_t = (a.T for a in (outer_gate, inner_gate, conv_input, conv_taps))
    recv, inner_t = lax.optimization_barrier((recv, inner_t))
    got = lax.all_gather(recv, TP)
    outer_f, inner_f, input_f, taps = (a.astype(F32) for a in (outer_t, inner_t, input_t, taps_t))
    mixed = inner_f * input_f
    before = lax.ppermute(mixed[:, -2:], "sp", [(i - 1, i) for i in range(1, groups)])
    padded = jnp.concatenate([before, mixed], axis=1)
    conv_sum = taps[:, 0:1] * padded[:, :-2] + taps[:, 1:2] * padded[:, 1:-1] + taps[:, 2:3] * padded[:, 2:]
    conv_out = (outer_f * conv_sum).astype(BF16)
    conv_all = lax.all_gather(conv_out, TP)

    rows = 2 * LANES
    full = lambda *dims: pl.BlockSpec(dims, lambda i, at: (0,) * len(dims))
    delta, hidden, own, other = call(
        functools.partial(expert_body, ys),
        (
            shape((slots, 2 * units), BF16),
            shape((slots, units), BF16),
            shape((ys, slots, LANES), BF16),
            shape((ys, slots, LANES), BF16),
        ),
        (10 * slots * width * units, 2**24),
        grid_spec=pltpu.PrefetchScalarGridSpec(
            num_scalar_prefetch=1,
            grid=(slots // rows,),
            in_specs=[
                pl.BlockSpec((tps, rows, 2 * LANES), lambda i, at: (0, i, 0)),
                full(width, units),
                full(width, units),
                full(units, width),
            ],
            out_specs=[
                pl.BlockSpec((rows, 2 * units), lambda i, at: (i, 0)),
                pl.BlockSpec((rows, units), lambda i, at: (i, 0)),
                pl.BlockSpec((ys, rows, LANES), lambda i, at: (0, i, 0)),
                pl.BlockSpec((ys, rows, LANES), lambda i, at: (0, i, 0)),
            ],
            scratch_shapes=[pltpu.VMEM((width, 2 * units), BF16)],
        ),
    )(core, got, gate_weight[0], up_weight[0], down_weight[0])
    partner = lax.ppermute(other, "c", swap)
    chip = (own.astype(F32) + partner.astype(F32)).astype(BF16)
    half_sums = lax.psum_scatter(chip, "y", scatter_dimension=0)

    fixed = lambda *dims: pl.BlockSpec(dims, lambda i: (0,) * len(dims))
    gate_grad, up_grad, down_grad = call(
        weight_body,
        (shape((width, units), BF16), shape((width, units), BF16), shape((units, width), BF16)),
        (6 * slots * width * units, 2**24),
        grid=(ys,),
        in_specs=[
            pl.BlockSpec((2, slots, 2 * LANES), lambda i: (i, 0, 0)),
            fixed(slots, 2 * units),
            fixed(slots, units),
        ],
        out_specs=[
            pl.BlockSpec((2 * LANES, units), lambda i: (i, 0)),
            pl.BlockSpec((2 * LANES, units), lambda i: (i, 0)),
            pl.BlockSpec((units, 2 * LANES), lambda i: (0, i)),
        ],
    )(got, delta, hidden)

    returned = lax.all_to_all(
        half_sums.reshape(groups, capacity, LANES), "sp", split_axis=0, concat_axis=0, tiled=True
    )
    stream_block, out_parts = call(
        token_body,
        (shape((tokens, LANES), BF16), shape((groups, channels // 2, LANES), BF16)),
        (2 * slots * tokens * LANES, 2**21),
        grid_spec=pltpu.PrefetchScalarGridSpec(
            num_scalar_prefetch=1,
            grid=(1,),
            in_specs=[whole(slots, LANES), whole(slots, LANES), block, whole(tps, channels, tokens)],
            out_specs=[whole(tokens, LANES), whole(groups, channels // 2, LANES)],
        ),
    )(at, returned.reshape(slots, LANES), select, cotangent, conv_all)

    out_tiles = lax.all_to_all(out_parts, "sp", split_axis=0, concat_axis=0, tiled=True)
    stream_all = lax.all_gather(stream_block, TP)
    outer_grad, scaled = call(
        functools.partial(conv_body, ys),
        (shape((channels, tokens), BF16), shape((channels, tokens), F32)),
        (2 * tokens * width * channels, 2**20),
        in_specs=[VMEM] * 4,
        out_specs=[VMEM] * 2,
    )(stream_all, out_weight.T, conv_sum, outer_t)
    later = lax.ppermute(scaled[:, :2], "sp", [(i, i - 1) for i in range(1, groups)])
    extended = jnp.concatenate([scaled, later], axis=1)
    mixed_grad = taps[:, 2:3] * extended[:, :-2] + taps[:, 1:2] * extended[:, 1:-1] + taps[:, 0:1] * extended[:, 2:]
    inner_grad = (mixed_grad * input_f).astype(BF16)
    input_grad = (mixed_grad * inner_f).astype(BF16)

    moves = [
        ((r * tps + j) * tps + t, (2 * t + r) * tps + j) for r in range(2) for j in range(tps) for t in range(tps)
    ]
    tile = lax.ppermute(out_tiles.astype(F32).sum(axis=0), ("sp", "y", "c"), moves)
    out_grad = jnp.concatenate([tile[:, :channels], tile[:, channels:]], axis=0)
    return (gate_grad[None], up_grad[None], down_grad[None], out_grad, outer_grad.T, inner_grad.T, input_grad.T)


def solution(mesh):
    groups, tps = mesh.devices.shape
    fine = Mesh(mesh.devices.reshape(groups, tps // 2, 2), ("sp", "y", "c"))
    placed = (
        P("sp", None),
        P("sp", None),
        P("sp", None),
        P("sp", None),
        P("sp", None, TP),
        P("sp", None, TP),
        P("sp", TP, None),
        P("sp", TP),
        P("sp", TP),
        P("sp", TP),
        P(None, TP),
        P(None, TP),
    )
    return jax.shard_map(
        per_device,
        mesh=fine,
        in_specs=placed,
        out_specs=(
            P("sp", None, TP),
            P("sp", None, TP),
            P("sp", TP, None),
            P("sp", TP),
            P("sp", TP),
            P("sp", TP),
            P("sp", TP),
        ),
        check_vma=False,
    )
```

```python
import functools

import jax
import jax.numpy as jnp
from jax import lax
from jax.experimental import pallas as pl
from jax.experimental.pallas import tpu as pltpu
from jax.sharding import Mesh, PartitionSpec as P

BF16, F32, I32 = jnp.bfloat16, jnp.float32, jnp.int32
TP = ("y", "c")
NT = (((1,), (1,)), ((), ()))
TN = (((0,), (0,)), ((), ()))
LANES = 128
VMEM = pl.BlockSpec(memory_space=pltpu.VMEM)


def mm(a, b, dims=None):
    if dims is None:
        return jnp.dot(a, b, preferred_element_type=F32)
    return lax.dot_general(a, b, dims, preferred_element_type=F32)


def call(body, out, cost, room=48 * 1024 * 1024, **kw):
    flops, moved = cost
    return pl.pallas_call(
        body,
        out_shape=out,
        cost_estimate=pl.CostEstimate(flops=flops, bytes_accessed=moved, transcendentals=0),
        compiler_params=pltpu.CompilerParams(vmem_limit_bytes=room),
        **kw,
    )


def shape(dims, kind):
    return jax.ShapeDtypeStruct(dims, kind)


def select_body(experts, capacity, at_ref, routes_ref, weights_ref, rows_ref, cot_ref, send_ref, select_ref):
    tokens = routes_ref.shape[1]
    number = lax.broadcasted_iota(I32, (experts, tokens), 0)
    first = routes_ref[0:1, :] == number
    second = routes_ref[1:2, :] == number
    hit = jnp.where(first | second, 1.0, 0.0).astype(F32)
    weight = jnp.where(first, weights_ref[0:1, :], jnp.where(second, weights_ref[1:2, :], 0.0))
    earlier = lax.broadcasted_iota(I32, (tokens, tokens), 0) < lax.broadcasted_iota(I32, (tokens, tokens), 1)
    place = mm(hit.astype(BF16), jnp.where(earlier, 1.0, 0.0).astype(BF16))
    place = jnp.where(hit > 0.0, place, -1.0)
    slot = lax.broadcasted_iota(I32, (capacity, tokens), 0).astype(F32)
    picked, scales = [], []
    for e in range(experts):
        one = jnp.where(slot == place[e : e + 1, :], 1.0, 0.0)
        scale = jnp.sum(one * weight[e : e + 1, :], axis=1, keepdims=True)
        picked += [one, one]
        scales += [scale, scale]
    select = jnp.concatenate(picked, axis=0).astype(BF16)
    scale = jnp.concatenate(scales, axis=0)
    select_ref[...] = select
    send_ref[:, :LANES] = mm(select, rows_ref[...]).astype(BF16)
    send_ref[:, LANES:] = (mm(select, cot_ref[...]) * scale).astype(BF16)


def share(delta, gate_ref, up_ref, y, c):
    picked = []
    for k in (y, y + 1):
        at = pl.ds(pl.multiple_of((2 * k + c) * LANES, LANES), LANES)
        picked.append(jnp.concatenate([gate_ref[at, :], up_ref[at, :]], axis=1))
    return mm(delta, jnp.concatenate(picked, axis=0), NT)


def expert_body(steps, core_ref, got_ref, gate_ref, up_ref, down_ref, delta_ref, hidden_ref, other_ref):
    rows = got_ref.shape[1]
    pre = jnp.zeros((rows, 2 * LANES), F32)
    back = jnp.zeros((rows, LANES), F32)
    for k in range(steps):
        ch = slice(k * 2 * LANES, (k + 1) * 2 * LANES)
        x = jnp.concatenate([got_ref[2 * k, :, :LANES], got_ref[2 * k + 1, :, :LANES]], axis=1)
        d = jnp.concatenate([got_ref[2 * k, :, LANES:], got_ref[2 * k + 1, :, LANES:]], axis=1)
        pre = pre + mm(x, jnp.concatenate([gate_ref[ch, :], up_ref[ch, :]], axis=1))
        back = back + mm(d, down_ref[:, ch], NT)
    gate, up = pre[:, :LANES], pre[:, LANES:]
    sigma = jax.nn.sigmoid(gate)
    silu = gate * sigma
    hidden_ref[...] = (silu * up).astype(BF16)
    delta = jnp.concatenate(
        [
            (back * up * sigma * (1.0 + gate * (1.0 - sigma))).astype(BF16),
            (back * silu).astype(BF16),
        ],
        axis=1,
    )
    delta_ref[...] = delta
    for y in range(0, steps, 2):
        part = share(delta, gate_ref, up_ref, y, 1 - core_ref[0]).astype(BF16)
        other_ref[y] = part[:, :LANES]
        other_ref[y + 1] = part[:, LANES:]


def chip_body(steps, core_ref, delta_ref, gate_ref, up_ref, partner_ref, chip_ref):
    delta = delta_ref[...]
    for y in range(0, steps, 2):
        part = share(delta, gate_ref, up_ref, y, core_ref[0])
        chip_ref[y] = (part[:, :LANES] + partner_ref[y].astype(F32)).astype(BF16)
        chip_ref[y + 1] = (part[:, LANES:] + partner_ref[y + 1].astype(F32)).astype(BF16)


def weight_body(got_ref, delta_ref, hidden_ref, gate_ref, up_ref, down_ref):
    x = jnp.concatenate([got_ref[0, :, :LANES], got_ref[1, :, :LANES]], axis=1)
    d = jnp.concatenate([got_ref[0, :, LANES:], got_ref[1, :, LANES:]], axis=1)
    grads = mm(x, delta_ref[...], TN)
    gate_ref[...] = grads[:, :LANES].astype(BF16)
    up_ref[...] = grads[:, LANES:].astype(BF16)
    down_ref[...] = mm(hidden_ref[...], d, TN).astype(BF16)


def token_body(at_ref, back_ref, select_ref, cot_ref, conv_ref, grad_ref, out_ref):
    moe = mm(select_ref[...], back_ref[...], TN).astype(BF16)
    grad = (cot_ref[...].astype(F32) + moe.astype(F32)).astype(BF16)
    grad_ref[0] = grad
    grad_ref[1] = grad
    flipped = grad.astype(F32).T.astype(BF16)
    count, width, tokens = conv_ref.shape
    half = width // 2
    left = jnp.concatenate([flipped[r * width : r * width + half] for r in range(2)], axis=0)
    right = jnp.concatenate([flipped[r * width + half : (r + 1) * width] for r in range(2)], axis=0)
    lhs = jnp.concatenate([left, right], axis=1)
    blank = jnp.zeros((width, tokens), BF16)
    for j in range(0, count, 2):
        rhs = []
        for k in (j, j + 1):
            rhs += [jnp.concatenate([conv_ref[k], blank], axis=1), jnp.concatenate([blank, conv_ref[k]], axis=1)]
        part = mm(lhs, jnp.concatenate(rhs, axis=0), NT).astype(BF16)
        for r in range(2):
            rows = part[r * half : (r + 1) * half]
            out_ref[r * count + j] = rows[:, :LANES]
            out_ref[r * count + j + 1] = rows[:, LANES:]


def conv_body(steps, grads_ref, weight_ref, sum_ref, outer_ref, outer_grad_ref, scaled_ref):
    total = jnp.zeros(sum_ref.shape, F32)
    for k in range(steps):
        g = jnp.concatenate([grads_ref[2 * k, 0], grads_ref[2 * k + 1, 0]], axis=1)
        total = total + mm(weight_ref[:, k * 2 * LANES : (k + 1) * 2 * LANES], g, NT)
    outer_grad_ref[...] = (total * sum_ref[...]).astype(BF16)
    scaled_ref[...] = total * outer_ref[...].astype(F32)


def per_device(
    cotangent,
    stream,
    routes,
    route_weights,
    gate_weight,
    up_weight,
    down_weight,
    outer_gate,
    inner_gate,
    conv_input,
    conv_taps,
    out_weight,
):
    groups = lax.axis_size("sp")
    ys = lax.axis_size("y")
    tps = 2 * ys
    experts = groups // 2
    tokens, width = stream.shape
    capacity = 3 * tokens // experts
    slots = groups * capacity
    units = gate_weight.shape[2]
    channels = outer_gate.shape[1]
    core = lax.axis_index("c").astype(I32).reshape(1)
    at = (2 * lax.axis_index("y") + lax.axis_index("c")).astype(I32).reshape(1)
    swap = [(0, 1), (1, 0)]

    block = pl.BlockSpec((tokens, LANES), lambda i, at: (0, at[0]))
    whole = lambda *dims: pl.BlockSpec(dims, lambda i, at: (0,) * len(dims))
    send, select = call(
        functools.partial(select_body, experts, capacity),
        (shape((slots, 2 * LANES), BF16), shape((slots, LANES), BF16)),
        (2 * slots * tokens * 2 * LANES, 2**20),
        room=67_043_328,
        grid_spec=pltpu.PrefetchScalarGridSpec(
            num_scalar_prefetch=1,
            grid=(1,),
            in_specs=[whole(2, tokens), whole(2, tokens), block, block],
            out_specs=[whole(slots, 2 * LANES), whole(slots, LANES)],
        ),
    )(at, routes.T, route_weights.T, stream, cotangent)
    recv = lax.all_to_all(
        send.reshape(groups, capacity, 2 * LANES), "sp", split_axis=0, concat_axis=0, tiled=True
    ).reshape(slots, 2 * LANES)

    outer_t, inner_t, input_t, taps_t = (a.T for a in (outer_gate, inner_gate, conv_input, conv_taps))
    recv, inner_t = lax.optimization_barrier((recv, inner_t))
    got = lax.all_gather(recv, TP)
    outer_f, inner_f, input_f, taps = (a.astype(F32) for a in (outer_t, inner_t, input_t, taps_t))
    mixed = inner_f * input_f
    before = lax.ppermute(mixed[:, -2:], "sp", [(i - 1, i) for i in range(1, groups)])
    padded = jnp.concatenate([before, mixed], axis=1)
    conv_sum = taps[:, 0:1] * padded[:, :-2] + taps[:, 1:2] * padded[:, 1:-1] + taps[:, 2:3] * padded[:, 2:]
    conv_out = (outer_f * conv_sum).astype(BF16)
    got, conv_out, conv_sum = lax.optimization_barrier((got, conv_out, conv_sum))

    rows = 2 * LANES
    full = lambda *dims: pl.BlockSpec(dims, lambda i, at: (0,) * len(dims))
    delta, hidden, other = call(
        functools.partial(expert_body, ys),
        (
            shape((slots, 2 * units), BF16),
            shape((slots, units), BF16),
            shape((ys, slots, LANES), BF16),
        ),
        (8 * slots * width * units, 2**24),
        grid_spec=pltpu.PrefetchScalarGridSpec(
            num_scalar_prefetch=1,
            grid=(slots // rows,),
            in_specs=[
                pl.BlockSpec((tps, rows, 2 * LANES), lambda i, at: (0, i, 0)),
                full(width, units),
                full(width, units),
                full(units, width),
            ],
            out_specs=[
                pl.BlockSpec((rows, 2 * units), lambda i, at: (i, 0)),
                pl.BlockSpec((rows, units), lambda i, at: (i, 0)),
                pl.BlockSpec((ys, rows, LANES), lambda i, at: (0, i, 0)),
            ],
        ),
    )(core, got, gate_weight[0], up_weight[0], down_weight[0])
    partner = lax.ppermute(other, "c", swap)
    chip = call(
        functools.partial(chip_body, ys),
        shape((ys, slots, LANES), BF16),
        (2 * slots * width * units, 2**22),
        grid_spec=pltpu.PrefetchScalarGridSpec(
            num_scalar_prefetch=1,
            grid=(slots // rows,),
            in_specs=[
                pl.BlockSpec((rows, 2 * units), lambda i, at: (i, 0)),
                full(width, units),
                full(width, units),
                pl.BlockSpec((ys, rows, LANES), lambda i, at: (0, i, 0)),
            ],
            out_specs=pl.BlockSpec((ys, rows, LANES), lambda i, at: (0, i, 0)),
        ),
    )(core, delta, gate_weight[0], up_weight[0], partner)
    chip, delta, conv_out = lax.optimization_barrier((chip, delta, conv_out))
    half_sums = lax.psum_scatter(chip, "y", scatter_dimension=0)
    conv_all = lax.all_gather(conv_out, TP)

    fixed = lambda *dims: pl.BlockSpec(dims, lambda i: (0,) * len(dims))
    gate_grad, up_grad, down_grad = call(
        weight_body,
        (shape((width, units), BF16), shape((width, units), BF16), shape((units, width), BF16)),
        (6 * slots * width * units, 2**24),
        grid=(ys,),
        in_specs=[
            pl.BlockSpec((2, slots, 2 * LANES), lambda i: (i, 0, 0)),
            fixed(slots, 2 * units),
            fixed(slots, units),
        ],
        out_specs=[
            pl.BlockSpec((2 * LANES, units), lambda i: (i, 0)),
            pl.BlockSpec((2 * LANES, units), lambda i: (i, 0)),
            pl.BlockSpec((units, 2 * LANES), lambda i: (0, i)),
        ],
    )(got, delta, hidden)

    half_sums, gate_grad, up_grad, down_grad, conv_all = lax.optimization_barrier(
        (half_sums, gate_grad, up_grad, down_grad, conv_all)
    )
    returned = lax.all_to_all(
        half_sums.reshape(groups, capacity, LANES), "sp", split_axis=0, concat_axis=0, tiled=True
    )
    stream_block, out_parts = call(
        token_body,
        (shape((2, tokens, LANES), BF16), shape((groups, channels // 2, LANES), BF16)),
        (2 * slots * tokens * LANES, 2**21),
        grid_spec=pltpu.PrefetchScalarGridSpec(
            num_scalar_prefetch=1,
            grid=(1,),
            in_specs=[whole(slots, LANES), whole(slots, LANES), block, whole(tps, channels, tokens)],
            out_specs=[whole(2, tokens, LANES), whole(groups, channels // 2, LANES)],
        ),
    )(at, returned.reshape(slots, LANES), select, cotangent, conv_all)

    out_tiles = lax.all_to_all(out_parts, "sp", split_axis=0, concat_axis=0, tiled=True)
    stream_all = lax.all_gather(stream_block, TP)
    outer_grad, scaled = call(
        functools.partial(conv_body, ys),
        (shape((channels, tokens), BF16), shape((channels, tokens), F32)),
        (2 * tokens * width * channels, 2**20),
        in_specs=[VMEM] * 4,
        out_specs=[VMEM] * 2,
    )(stream_all, out_weight.T, conv_sum, outer_t)
    later = lax.ppermute(scaled[:, :2], "sp", [(i, i - 1) for i in range(1, groups)])
    extended = jnp.concatenate([scaled, later], axis=1)
    mixed_grad = taps[:, 2:3] * extended[:, :-2] + taps[:, 1:2] * extended[:, 1:-1] + taps[:, 0:1] * extended[:, 2:]
    inner_grad = (mixed_grad * input_f).astype(BF16)
    input_grad = (mixed_grad * inner_f).astype(BF16)

    moves = [
        ((r * tps + j) * tps + t, (2 * t + r) * tps + j) for r in range(2) for j in range(tps) for t in range(tps)
    ]
    tile = lax.ppermute(out_tiles.astype(F32).sum(axis=0), ("sp", "y", "c"), moves)
    out_grad = jnp.concatenate([tile[:, :channels], tile[:, channels:]], axis=0)
    return (gate_grad[None], up_grad[None], down_grad[None], out_grad, outer_grad.T, inner_grad.T, input_grad.T)


def solution(mesh):
    groups, tps = mesh.devices.shape
    fine = Mesh(mesh.devices.reshape(groups, tps // 2, 2), ("sp", "y", "c"))
    placed = (
        P("sp", None),
        P("sp", None),
        P("sp", None),
        P("sp", None),
        P("sp", None, TP),
        P("sp", None, TP),
        P("sp", TP, None),
        P("sp", TP),
        P("sp", TP),
        P("sp", TP),
        P(None, TP),
        P(None, TP),
    )
    return jax.shard_map(
        per_device,
        mesh=fine,
        in_specs=placed,
        out_specs=(
            P("sp", None, TP),
            P("sp", None, TP),
            P("sp", TP, None),
            P("sp", TP),
            P("sp", TP),
            P("sp", TP),
            P("sp", TP),
        ),
        check_vma=False,
    )
```

```python
import functools

import jax
import jax.numpy as jnp
from jax import lax
from jax.experimental import pallas as pl
from jax.experimental.pallas import tpu as pltpu
from jax.sharding import Mesh, PartitionSpec as P

BF16, F32, I32 = jnp.bfloat16, jnp.float32, jnp.int32
TP = ("y", "c")
NT = (((1,), (1,)), ((), ()))
TN = (((0,), (0,)), ((), ()))
LANES = 128
VMEM = pl.BlockSpec(memory_space=pltpu.VMEM)


def mm(a, b, dims=None):
    if dims is None:
        return jnp.dot(a, b, preferred_element_type=F32)
    return lax.dot_general(a, b, dims, preferred_element_type=F32)


def call(body, out, cost, room=48 * 1024 * 1024, **kw):
    flops, moved = cost
    return pl.pallas_call(
        body,
        out_shape=out,
        cost_estimate=pl.CostEstimate(flops=flops, bytes_accessed=moved, transcendentals=0),
        compiler_params=pltpu.CompilerParams(vmem_limit_bytes=room),
        **kw,
    )


def shape(dims, kind):
    return jax.ShapeDtypeStruct(dims, kind)


def select_body(experts, capacity, at_ref, routes_ref, weights_ref, rows_ref, cot_ref, send_ref, select_ref):
    tokens = routes_ref.shape[1]
    number = lax.broadcasted_iota(I32, (experts, tokens), 0)
    first = routes_ref[0:1, :] == number
    second = routes_ref[1:2, :] == number
    hit = jnp.where(first | second, 1.0, 0.0).astype(F32)
    weight = jnp.where(first, weights_ref[0:1, :], jnp.where(second, weights_ref[1:2, :], 0.0))
    earlier = lax.broadcasted_iota(I32, (tokens, tokens), 0) < lax.broadcasted_iota(I32, (tokens, tokens), 1)
    place = mm(hit.astype(BF16), jnp.where(earlier, 1.0, 0.0).astype(BF16))
    place = jnp.where(hit > 0.0, place, -1.0)
    slot = lax.broadcasted_iota(I32, (capacity, tokens), 0).astype(F32)
    picked, scales = [], []
    for e in range(experts):
        one = jnp.where(slot == place[e : e + 1, :], 1.0, 0.0)
        scale = jnp.sum(one * weight[e : e + 1, :], axis=1, keepdims=True)
        picked += [one, one]
        scales += [scale, scale]
    select = jnp.concatenate(picked, axis=0).astype(BF16)
    scale = jnp.concatenate(scales, axis=0)
    select_ref[...] = select
    send_ref[:, :LANES] = mm(select, rows_ref[...]).astype(BF16)
    send_ref[:, LANES:] = (mm(select, cot_ref[...]) * scale).astype(BF16)


def expert_body(steps, got_ref, gate_ref, up_ref, down_ref, delta_ref, hidden_ref):
    rows = got_ref.shape[1]
    pre = jnp.zeros((rows, 2 * LANES), F32)
    back = jnp.zeros((rows, LANES), F32)
    for k in range(steps):
        ch = slice(k * 2 * LANES, (k + 1) * 2 * LANES)
        x = jnp.concatenate([got_ref[2 * k, :, :LANES], got_ref[2 * k + 1, :, :LANES]], axis=1)
        d = jnp.concatenate([got_ref[2 * k, :, LANES:], got_ref[2 * k + 1, :, LANES:]], axis=1)
        pre = pre + mm(x, jnp.concatenate([gate_ref[ch, :], up_ref[ch, :]], axis=1))
        back = back + mm(d, down_ref[:, ch], NT)
    gate, up = pre[:, :LANES], pre[:, LANES:]
    sigma = jax.nn.sigmoid(gate)
    silu = gate * sigma
    hidden_ref[...] = (silu * up).astype(BF16)
    delta_ref[:, :LANES] = (back * up * sigma * (1.0 + gate * (1.0 - sigma))).astype(BF16)
    delta_ref[:, LANES:] = (back * silu).astype(BF16)


def chip_body(steps, own_ref, partner_ref, own_weight_ref, partner_weight_ref, chip_ref):
    delta = jnp.concatenate([own_ref[...], partner_ref[...]], axis=1)
    for y in range(0, steps, 2):
        weight = [jnp.concatenate([own_weight_ref[k], partner_weight_ref[k]], axis=1) for k in (y, y + 1)]
        part = mm(delta, jnp.concatenate(weight, axis=0), NT).astype(BF16)
        chip_ref[y] = part[:, :LANES]
        chip_ref[y + 1] = part[:, LANES:]


def weight_body(got_ref, delta_ref, hidden_ref, gate_ref, up_ref, down_ref):
    x = jnp.concatenate([got_ref[0, :, :LANES], got_ref[1, :, :LANES]], axis=1)
    d = jnp.concatenate([got_ref[0, :, LANES:], got_ref[1, :, LANES:]], axis=1)
    grads = mm(x, delta_ref[...], TN)
    gate_ref[...] = grads[:, :LANES].astype(BF16)
    up_ref[...] = grads[:, LANES:].astype(BF16)
    down_ref[...] = mm(hidden_ref[...], d, TN).astype(BF16)


def token_body(at_ref, back_ref, select_ref, cot_ref, grad_ref):
    moe = mm(select_ref[...], back_ref[...], TN).astype(BF16)
    grad_ref[...] = (cot_ref[...].astype(F32) + moe.astype(F32)).astype(BF16)


def conv_body(steps, grads_ref, weight_ref, conv_ref, sum_ref, outer_ref, outer_grad_ref, scaled_ref, out_ref):
    total = jnp.zeros(sum_ref.shape, F32)
    half = conv_ref.shape[0] // 2
    low = lax.broadcasted_iota(I32, (half, LANES), 1) < LANES // 2
    for k in range(steps):
        g = jnp.concatenate([grads_ref[2 * k], grads_ref[2 * k + 1]], axis=1)
        total = total + mm(weight_ref[:, k * 2 * LANES : (k + 1) * 2 * LANES], g, NT)
        parts = mm(conv_ref[...], g)
        for t in range(2):
            top, bottom = (parts[r * half : (r + 1) * half, t * LANES : (t + 1) * LANES] for r in range(2))
            out_ref[4 * k + 2 * t] = jnp.where(low, top, pltpu.roll(bottom, LANES // 2, 1)).astype(BF16)
            out_ref[4 * k + 2 * t + 1] = jnp.where(low, pltpu.roll(top, LANES // 2, 1), bottom).astype(BF16)
    outer_grad_ref[...] = (total * sum_ref[...]).astype(BF16)
    scaled_ref[...] = total * outer_ref[...].astype(F32)


def out_body(tiles_ref, out_ref):
    total = tiles_ref[0].astype(F32)
    for s in range(1, tiles_ref.shape[0]):
        total = total + tiles_ref[s].astype(F32)
    half = LANES // 2
    out_ref[...] = jnp.concatenate([total[:, :half], total[:, half:]], axis=0).T


def per_device(
    cotangent,
    stream,
    routes,
    route_weights,
    gate_weight,
    up_weight,
    down_weight,
    outer_gate,
    inner_gate,
    conv_input,
    conv_taps,
    out_weight,
):
    groups = lax.axis_size("sp")
    ys = lax.axis_size("y")
    tps = 2 * ys
    experts = groups // 2
    tokens, width = stream.shape
    capacity = 3 * tokens // experts
    slots = groups * capacity
    units = gate_weight.shape[2]
    channels = outer_gate.shape[1]
    core = lax.axis_index("c").astype(I32).reshape(1)
    at = (2 * lax.axis_index("y") + lax.axis_index("c")).astype(I32).reshape(1)
    swap = [(0, 1), (1, 0)]

    block = pl.BlockSpec((tokens, LANES), lambda i, at: (0, at[0]))
    whole = lambda *dims: pl.BlockSpec(dims, lambda i, at: (0,) * len(dims))
    send, select = call(
        functools.partial(select_body, experts, capacity),
        (shape((slots, 2 * LANES), BF16), shape((slots, LANES), BF16)),
        (2 * slots * tokens * 2 * LANES, 2**20),
        room=67_043_328,
        grid_spec=pltpu.PrefetchScalarGridSpec(
            num_scalar_prefetch=1,
            grid=(1,),
            in_specs=[whole(2, tokens), whole(2, tokens), block, block],
            out_specs=[whole(slots, 2 * LANES), whole(slots, LANES)],
        ),
    )(at, routes.T, route_weights.T, stream, cotangent)
    recv = lax.all_to_all(
        send.reshape(groups, capacity, 2 * LANES), "sp", split_axis=0, concat_axis=0, tiled=True
    ).reshape(slots, 2 * LANES)

    outer_t, inner_t, input_t, taps_t = (a.T for a in (outer_gate, inner_gate, conv_input, conv_taps))
    recv, inner_t, gate_in, up_in = lax.optimization_barrier((recv, inner_t, gate_weight[0], up_weight[0]))
    got = lax.all_gather(recv, TP)
    by_core = jnp.concatenate([gate_in, up_in], axis=1).reshape(ys, 2, LANES, 2 * units)
    own_weight = lax.dynamic_index_in_dim(by_core, core[0], 1, keepdims=False)
    partner_weight = lax.ppermute(lax.dynamic_index_in_dim(by_core, 1 - core[0], 1, keepdims=False), "c", swap)
    outer_f, inner_f, input_f, taps = (a.astype(F32) for a in (outer_t, inner_t, input_t, taps_t))
    mixed = inner_f * input_f
    before = lax.ppermute(mixed[:, -2:], "sp", [(i - 1, i) for i in range(1, groups)])
    padded = jnp.concatenate([before, mixed], axis=1)
    conv_sum = taps[:, 0:1] * padded[:, :-2] + taps[:, 1:2] * padded[:, 1:-1] + taps[:, 2:3] * padded[:, 2:]
    conv_out = (outer_f * conv_sum).astype(BF16)
    got, conv_out, conv_sum, own_weight, partner_weight = lax.optimization_barrier(
        (got, conv_out, conv_sum, own_weight, partner_weight)
    )

    rows = 2 * LANES
    fixed = lambda *dims: pl.BlockSpec(dims, lambda i: (0,) * len(dims))
    delta_block = pl.BlockSpec((rows, 2 * units), lambda i: (i, 0))
    delta, hidden = call(
        functools.partial(expert_body, ys),
        (shape((slots, 2 * units), BF16), shape((slots, units), BF16)),
        (6 * slots * width * units, 2**24),
        grid=(slots // rows,),
        in_specs=[
            pl.BlockSpec((tps, rows, 2 * LANES), lambda i: (0, i, 0)),
            fixed(width, units),
            fixed(width, units),
            fixed(units, width),
        ],
        out_specs=[delta_block, pl.BlockSpec((rows, units), lambda i: (i, 0))],
    )(got, gate_weight[0], up_weight[0], down_weight[0])
    chip = call(
        functools.partial(chip_body, ys),
        shape((ys, slots, LANES), BF16),
        (4 * slots * width * units, 2**22),
        grid=(slots // rows,),
        in_specs=[delta_block, delta_block, fixed(ys, LANES, 2 * units), fixed(ys, LANES, 2 * units)],
        out_specs=pl.BlockSpec((ys, rows, LANES), lambda i: (0, i, 0)),
    )(delta, lax.ppermute(delta, "c", swap), own_weight, partner_weight)
    chip, delta = lax.optimization_barrier((chip, delta))
    half_sums = lax.psum_scatter(chip, "y", scatter_dimension=0)

    gate_grad, up_grad, down_grad = call(
        weight_body,
        (shape((width, units), BF16), shape((width, units), BF16), shape((units, width), BF16)),
        (6 * slots * width * units, 2**24),
        grid=(ys,),
        in_specs=[
            pl.BlockSpec((2, slots, 2 * LANES), lambda i: (i, 0, 0)),
            fixed(slots, 2 * units),
            fixed(slots, units),
        ],
        out_specs=[
            pl.BlockSpec((2 * LANES, units), lambda i: (i, 0)),
            pl.BlockSpec((2 * LANES, units), lambda i: (i, 0)),
            pl.BlockSpec((units, 2 * LANES), lambda i: (0, i)),
        ],
    )(got, delta, hidden)

    half_sums, gate_grad, up_grad, down_grad = lax.optimization_barrier((half_sums, gate_grad, up_grad, down_grad))
    returned = lax.all_to_all(
        half_sums.reshape(groups, capacity, LANES), "sp", split_axis=0, concat_axis=0, tiled=True
    )
    stream_block = call(
        token_body,
        shape((tokens, LANES), BF16),
        (2 * slots * tokens * LANES, 2**21),
        grid_spec=pltpu.PrefetchScalarGridSpec(
            num_scalar_prefetch=1,
            grid=(1,),
            in_specs=[whole(slots, LANES), whole(slots, LANES), block],
            out_specs=whole(tokens, LANES),
        ),
    )(at, returned.reshape(slots, LANES), select, cotangent)
    outer_grad, scaled, out_parts = call(
        functools.partial(conv_body, ys),
        (
            shape((channels, tokens), BF16),
            shape((channels, tokens), F32),
            shape((groups, channels // 2, LANES), BF16),
        ),
        (4 * tokens * width * channels, 2**20),
        in_specs=[VMEM] * 5,
        out_specs=[VMEM] * 3,
    )(lax.all_gather(stream_block, TP), out_weight.T, conv_out, conv_sum, outer_t)
    out_tiles = lax.all_to_all(out_parts, "sp", split_axis=0, concat_axis=0, tiled=True)
    out_grad = call(
        out_body,
        shape((channels, width // groups), F32),
        (2**17, 2**19),
        in_specs=[VMEM],
        out_specs=VMEM,
    )(out_tiles)
    later = lax.ppermute(scaled[:, :2], "sp", [(i, i - 1) for i in range(1, groups)])
    extended = jnp.concatenate([scaled, later], axis=1)
    mixed_grad = taps[:, 2:3] * extended[:, :-2] + taps[:, 1:2] * extended[:, 1:-1] + taps[:, 0:1] * extended[:, 2:]
    inner_grad = (mixed_grad * input_f).astype(BF16)
    input_grad = (mixed_grad * inner_f).astype(BF16)
    return (gate_grad[None], up_grad[None], down_grad[None], out_grad, outer_grad.T, inner_grad.T, input_grad.T)


def solution(mesh):
    groups, tps = mesh.devices.shape
    fine = Mesh(mesh.devices.reshape(groups, tps // 2, 2), ("sp", "y", "c"))
    placed = (
        P("sp", None),
        P("sp", None),
        P("sp", None),
        P("sp", None),
        P("sp", None, TP),
        P("sp", None, TP),
        P("sp", TP, None),
        P("sp", TP),
        P("sp", TP),
        P("sp", TP),
        P(None, TP),
        P(None, TP),
    )
    return jax.shard_map(
        per_device,
        mesh=fine,
        in_specs=placed,
        out_specs=(
            P("sp", None, TP),
            P("sp", None, TP),
            P("sp", TP, None),
            P("sp", TP),
            P("sp", TP),
            P("sp", TP),
            P("sp", TP),
        ),
        check_vma=False,
    )
```

```python
import functools

import jax
import jax.numpy as jnp
from jax import lax
from jax.experimental import pallas as pl
from jax.experimental.pallas import tpu as pltpu
from jax.sharding import Mesh, PartitionSpec as P

BF16, F32, I32 = jnp.bfloat16, jnp.float32, jnp.int32
TP = ("y", "c")
NT = (((1,), (1,)), ((), ()))
TN = (((0,), (0,)), ((), ()))
LANES = 128
VMEM = pl.BlockSpec(memory_space=pltpu.VMEM)


def mm(a, b, dims=None):
    if dims is None:
        return jnp.dot(a, b, preferred_element_type=F32)
    return lax.dot_general(a, b, dims, preferred_element_type=F32)


def call(body, out, cost, room=48 * 1024 * 1024, **kw):
    flops, moved = cost
    return pl.pallas_call(
        body,
        out_shape=out,
        cost_estimate=pl.CostEstimate(flops=flops, bytes_accessed=moved, transcendentals=0),
        compiler_params=pltpu.CompilerParams(vmem_limit_bytes=room),
        **kw,
    )


def shape(dims, kind):
    return jax.ShapeDtypeStruct(dims, kind)


def select_body(experts, capacity, at_ref, routes_ref, weights_ref, rows_ref, cot_ref, send_ref, select_ref):
    tokens = routes_ref.shape[1]
    number = lax.broadcasted_iota(I32, (experts, tokens), 0)
    first = routes_ref[0:1, :] == number
    second = routes_ref[1:2, :] == number
    hit = jnp.where(first | second, 1.0, 0.0).astype(F32)
    weight = jnp.where(first, weights_ref[0:1, :], jnp.where(second, weights_ref[1:2, :], 0.0))
    earlier = lax.broadcasted_iota(I32, (tokens, tokens), 0) < lax.broadcasted_iota(I32, (tokens, tokens), 1)
    place = mm(hit.astype(BF16), jnp.where(earlier, 1.0, 0.0).astype(BF16))
    place = jnp.where(hit > 0.0, place, -1.0)
    slot = lax.broadcasted_iota(I32, (capacity, tokens), 0).astype(F32)
    picked, scales = [], []
    for e in range(experts):
        one = jnp.where(slot == place[e : e + 1, :], 1.0, 0.0)
        scale = jnp.sum(one * weight[e : e + 1, :], axis=1, keepdims=True)
        picked += [one, one]
        scales += [scale, scale]
    select = jnp.concatenate(picked, axis=0).astype(BF16)
    scale = jnp.concatenate(scales, axis=0)
    select_ref[...] = select
    send_ref[:, :LANES] = mm(select, rows_ref[...]).astype(BF16)
    send_ref[:, LANES:] = (mm(select, cot_ref[...]) * scale).astype(BF16)


def layout_body(core_ref, gate_ref, up_ref, down_ref, gate2_ref, up2_ref, down2_ref, fore_ref, back_ref, rows_ref):
    for i, ref in enumerate((gate_ref, up_ref, gate2_ref, up2_ref)):
        fore_ref[:, i * LANES : (i + 1) * LANES] = ref[...]
    for k in range(back_ref.shape[0] // LANES):
        at = slice(k * LANES, (k + 1) * LANES)
        back_ref[at, :LANES] = down_ref[:, at].astype(F32).T.astype(BF16)
        back_ref[at, LANES:] = down2_ref[:, at].astype(F32).T.astype(BF16)
    for y in range(2 * rows_ref.shape[0]):
        at = pl.ds(pl.multiple_of((2 * y + core_ref[0]) * LANES, LANES), LANES)
        to = slice(y % 2 * LANES, (y % 2 + 1) * LANES)
        for i, ref in enumerate((gate_ref, up_ref, gate2_ref, up2_ref)):
            rows_ref[y // 2, i * LANES : (i + 1) * LANES, to] = ref[at, :].astype(F32).T.astype(BF16)


def expert_body(count, got_ref, fore_ref, back_ref, rows_ref, delta_ref, hidden_ref, chip_ref):
    x = jnp.concatenate([got_ref[t, :, :LANES] for t in range(count)], axis=1)
    pre = mm(x, fore_ref[...])
    d = jnp.concatenate([got_ref[t, :, LANES:] for t in range(count)], axis=1)
    back = mm(d, back_ref[...])
    deltas = []
    for i in range(2):
        gate = pre[:, 2 * i * LANES : (2 * i + 1) * LANES]
        up = pre[:, (2 * i + 1) * LANES : (2 * i + 2) * LANES]
        grad = back[:, i * LANES : (i + 1) * LANES]
        sigma = jax.nn.sigmoid(gate)
        silu = gate * sigma
        if i == 0:
            hidden_ref[...] = (silu * up).astype(BF16)
        deltas.append((grad * up * sigma * (1.0 + gate * (1.0 - sigma))).astype(BF16))
        deltas.append((grad * silu).astype(BF16))
    delta_ref[:, :LANES] = deltas[0]
    delta_ref[:, LANES:] = deltas[1]
    delta = jnp.concatenate(deltas, axis=1)
    for k in range(count // 4):
        part = mm(delta, rows_ref[k]).astype(BF16)
        chip_ref[2 * k] = part[:, :LANES]
        chip_ref[2 * k + 1] = part[:, LANES:]


def weight_body(got_ref, delta_ref, hidden_ref, gate_ref, up_ref, down_ref):
    x = jnp.concatenate([got_ref[0, :, :LANES], got_ref[1, :, :LANES]], axis=1)
    d = jnp.concatenate([got_ref[0, :, LANES:], got_ref[1, :, LANES:]], axis=1)
    grads = mm(x, delta_ref[...], TN)
    gate_ref[...] = grads[:, :LANES].astype(BF16)
    up_ref[...] = grads[:, LANES:].astype(BF16)
    down_ref[...] = mm(hidden_ref[...], d, TN).astype(BF16)


def token_body(at_ref, back_ref, select_ref, cot_ref, grad_ref):
    moe = mm(select_ref[...], back_ref[...], TN).astype(BF16)
    grad_ref[...] = (cot_ref[...].astype(F32) + moe.astype(F32)).astype(BF16)


def conv_body(steps, grads_ref, weight_ref, conv_ref, sum_ref, outer_ref, outer_grad_ref, scaled_ref, out_ref):
    total = jnp.zeros(sum_ref.shape, F32)
    half = conv_ref.shape[0] // 2
    low = lax.broadcasted_iota(I32, (half, LANES), 1) < LANES // 2
    for k in range(steps):
        g = jnp.concatenate([grads_ref[2 * k], grads_ref[2 * k + 1]], axis=1)
        total = total + mm(weight_ref[:, k * 2 * LANES : (k + 1) * 2 * LANES], g, NT)
        parts = mm(conv_ref[...], g)
        for t in range(2):
            top, bottom = (parts[r * half : (r + 1) * half, t * LANES : (t + 1) * LANES] for r in range(2))
            out_ref[4 * k + 2 * t] = jnp.where(low, top, pltpu.roll(bottom, LANES // 2, 1)).astype(BF16)
            out_ref[4 * k + 2 * t + 1] = jnp.where(low, pltpu.roll(top, LANES // 2, 1), bottom).astype(BF16)
    outer_grad_ref[...] = (total * sum_ref[...]).astype(BF16)
    scaled_ref[...] = total * outer_ref[...].astype(F32)


def out_body(tiles_ref, out_ref):
    total = tiles_ref[0].astype(F32)
    for s in range(1, tiles_ref.shape[0]):
        total = total + tiles_ref[s].astype(F32)
    half = LANES // 2
    out_ref[...] = jnp.concatenate([total[:, :half], total[:, half:]], axis=0).T


def per_device(
    cotangent,
    stream,
    routes,
    route_weights,
    gate_weight,
    up_weight,
    down_weight,
    outer_gate,
    inner_gate,
    conv_input,
    conv_taps,
    out_weight,
):
    groups = lax.axis_size("sp")
    ys = lax.axis_size("y")
    tps = 2 * ys
    experts = groups // 2
    tokens, width = stream.shape
    capacity = 3 * tokens // experts
    slots = groups * capacity
    units = gate_weight.shape[2]
    channels = outer_gate.shape[1]
    core = lax.axis_index("c").astype(I32).reshape(1)
    at = (2 * lax.axis_index("y") + lax.axis_index("c")).astype(I32).reshape(1)
    swap = [(0, 1), (1, 0)]

    block = pl.BlockSpec((tokens, LANES), lambda i, at: (0, at[0]))
    whole = lambda *dims: pl.BlockSpec(dims, lambda i, at: (0,) * len(dims))
    send, select = call(
        functools.partial(select_body, experts, capacity),
        (shape((slots, 2 * LANES), BF16), shape((slots, LANES), BF16)),
        (2 * slots * tokens * 2 * LANES, 2**20),
        room=67_043_328,
        grid_spec=pltpu.PrefetchScalarGridSpec(
            num_scalar_prefetch=1,
            grid=(1,),
            in_specs=[whole(2, tokens), whole(2, tokens), block, block],
            out_specs=[whole(slots, 2 * LANES), whole(slots, LANES)],
        ),
    )(at, routes.T, route_weights.T, stream, cotangent)
    recv = lax.all_to_all(
        send.reshape(groups, capacity, 2 * LANES), "sp", split_axis=0, concat_axis=0, tiled=True
    ).reshape(slots, 2 * LANES)

    outer_t, inner_t, input_t, taps_t = (a.T for a in (outer_gate, inner_gate, conv_input, conv_taps))
    weights = (gate_weight[0], up_weight[0], down_weight[0])
    recv, inner_t, *held = lax.optimization_barrier((recv, inner_t, *weights))
    got = lax.all_gather(recv, TP)
    laid = call(
        layout_body,
        (shape((width, 4 * units), BF16), shape((width, 2 * units), BF16), shape((ys // 2, 4 * units, 2 * LANES), BF16)),
        (2**22, 2**23),
        in_specs=[pl.BlockSpec(memory_space=pltpu.SMEM)] + [VMEM] * 6,
        out_specs=[VMEM] * 3,
    )(core, *held, *(lax.ppermute(a, "c", swap) for a in held))
    outer_f, inner_f, input_f, taps = (a.astype(F32) for a in (outer_t, inner_t, input_t, taps_t))
    mixed = inner_f * input_f
    before = lax.ppermute(mixed[:, -2:], "sp", [(i - 1, i) for i in range(1, groups)])
    padded = jnp.concatenate([before, mixed], axis=1)
    conv_sum = taps[:, 0:1] * padded[:, :-2] + taps[:, 1:2] * padded[:, 1:-1] + taps[:, 2:3] * padded[:, 2:]
    conv_out = (outer_f * conv_sum).astype(BF16)
    got, conv_out, conv_sum, laid = lax.optimization_barrier((got, conv_out, conv_sum, laid))

    rows = 2 * LANES
    fixed = lambda *dims: pl.BlockSpec(dims, lambda i: (0,) * len(dims))
    delta, hidden, chip = call(
        functools.partial(expert_body, tps),
        (shape((slots, 2 * units), BF16), shape((slots, units), BF16), shape((ys, slots, LANES), BF16)),
        (16 * slots * width * units, 2**24),
        grid=(slots // rows,),
        in_specs=[
            pl.BlockSpec((tps, rows, 2 * LANES), lambda i: (0, i, 0)),
            fixed(width, 4 * units),
            fixed(width, 2 * units),
            fixed(ys // 2, 4 * units, 2 * LANES),
        ],
        out_specs=[
            pl.BlockSpec((rows, 2 * units), lambda i: (i, 0)),
            pl.BlockSpec((rows, units), lambda i: (i, 0)),
            pl.BlockSpec((ys, rows, LANES), lambda i: (0, i, 0)),
        ],
    )(got, *laid)
    chip, delta = lax.optimization_barrier((chip, delta))
    half_sums = lax.psum_scatter(chip, "y", scatter_dimension=0)

    gate_grad, up_grad, down_grad = call(
        weight_body,
        (shape((width, units), BF16), shape((width, units), BF16), shape((units, width), BF16)),
        (6 * slots * width * units, 2**24),
        grid=(ys,),
        in_specs=[
            pl.BlockSpec((2, slots, 2 * LANES), lambda i: (i, 0, 0)),
            fixed(slots, 2 * units),
            fixed(slots, units),
        ],
        out_specs=[
            pl.BlockSpec((2 * LANES, units), lambda i: (i, 0)),
            pl.BlockSpec((2 * LANES, units), lambda i: (i, 0)),
            pl.BlockSpec((units, 2 * LANES), lambda i: (0, i)),
        ],
    )(got, delta, hidden)

    half_sums, gate_grad, up_grad, down_grad = lax.optimization_barrier((half_sums, gate_grad, up_grad, down_grad))
    returned = lax.all_to_all(
        half_sums.reshape(groups, capacity, LANES), "sp", split_axis=0, concat_axis=0, tiled=True
    )
    stream_block = call(
        token_body,
        shape((tokens, LANES), BF16),
        (2 * slots * tokens * LANES, 2**21),
        grid_spec=pltpu.PrefetchScalarGridSpec(
            num_scalar_prefetch=1,
            grid=(1,),
            in_specs=[whole(slots, LANES), whole(slots, LANES), block],
            out_specs=whole(tokens, LANES),
        ),
    )(at, returned.reshape(slots, LANES), select, cotangent)
    outer_grad, scaled, out_parts = call(
        functools.partial(conv_body, ys),
        (
            shape((channels, tokens), BF16),
            shape((channels, tokens), F32),
            shape((groups, channels // 2, LANES), BF16),
        ),
        (4 * tokens * width * channels, 2**20),
        in_specs=[VMEM] * 5,
        out_specs=[VMEM] * 3,
    )(lax.all_gather(stream_block, TP), out_weight.T, conv_out, conv_sum, outer_t)
    out_tiles = lax.all_to_all(out_parts, "sp", split_axis=0, concat_axis=0, tiled=True)
    out_grad = call(
        out_body,
        shape((channels, width // groups), F32),
        (2**17, 2**19),
        in_specs=[VMEM],
        out_specs=VMEM,
    )(out_tiles)
    later = lax.ppermute(scaled[:, :2], "sp", [(i, i - 1) for i in range(1, groups)])
    extended = jnp.concatenate([scaled, later], axis=1)
    mixed_grad = taps[:, 2:3] * extended[:, :-2] + taps[:, 1:2] * extended[:, 1:-1] + taps[:, 0:1] * extended[:, 2:]
    inner_grad = (mixed_grad * input_f).astype(BF16)
    input_grad = (mixed_grad * inner_f).astype(BF16)
    return (gate_grad[None], up_grad[None], down_grad[None], out_grad, outer_grad.T, inner_grad.T, input_grad.T)


def solution(mesh):
    groups, tps = mesh.devices.shape
    fine = Mesh(mesh.devices.reshape(groups, tps // 2, 2), ("sp", "y", "c"))
    placed = (
        P("sp", None),
        P("sp", None),
        P("sp", None),
        P("sp", None),
        P("sp", None, TP),
        P("sp", None, TP),
        P("sp", TP, None),
        P("sp", TP),
        P("sp", TP),
        P("sp", TP),
        P(None, TP),
        P(None, TP),
    )
    return jax.shard_map(
        per_device,
        mesh=fine,
        in_specs=placed,
        out_specs=(
            P("sp", None, TP),
            P("sp", None, TP),
            P("sp", TP, None),
            P("sp", TP),
            P("sp", TP),
            P("sp", TP),
            P("sp", TP),
        ),
        check_vma=False,
    )
```

```python
import functools

import jax
import jax.numpy as jnp
from jax import lax
from jax.experimental import pallas as pl
from jax.experimental.pallas import tpu as pltpu
from jax.sharding import Mesh, PartitionSpec as P


BF16, F32, I32 = jnp.bfloat16, jnp.float32, jnp.int32
TP = ("y", "c")
NT = (((1,), (1,)), ((), ()))
TN = (((0,), (0,)), ((), ()))
LANES = 128
VMEM = pl.BlockSpec(memory_space=pltpu.VMEM)


def mm(a, b, dims=None):
    if dims is None:
        return jnp.dot(a, b, preferred_element_type=F32)
    return lax.dot_general(a, b, dims, preferred_element_type=F32)


def call(body, out, cost, room=48 * 1024 * 1024, **kw):
    flops, moved = cost
    return pl.pallas_call(
        body,
        out_shape=out,
        cost_estimate=pl.CostEstimate(flops=flops, bytes_accessed=moved, transcendentals=0),
        compiler_params=pltpu.CompilerParams(vmem_limit_bytes=room),
        **kw,
    )


def shape(dims, kind):
    return jax.ShapeDtypeStruct(dims, kind)


def select_body(experts, capacity, at_ref, routes_ref, weights_ref, rows_ref, cot_ref, send_ref, select_ref, held, sems):
    at = pl.ds(pl.multiple_of(at_ref[0] * LANES, LANES), LANES)
    copies = [
        pltpu.make_async_copy(ref.at[:, at], held.at[i], sems.at[i]) for i, ref in enumerate((rows_ref, cot_ref))
    ]
    for copy in copies:
        copy.start()
    tokens = routes_ref.shape[1]
    number = lax.broadcasted_iota(I32, (experts, tokens), 0)
    first = routes_ref[0:1, :] == number
    second = routes_ref[1:2, :] == number
    hit = jnp.where(first | second, 1.0, 0.0).astype(F32)
    weight = jnp.where(first, weights_ref[0:1, :], jnp.where(second, weights_ref[1:2, :], 0.0))
    earlier = lax.broadcasted_iota(I32, (tokens, tokens), 0) < lax.broadcasted_iota(I32, (tokens, tokens), 1)
    place = mm(hit.astype(BF16), jnp.where(earlier, 1.0, 0.0).astype(BF16))
    place = jnp.where(hit > 0.0, place, -1.0)
    slot = lax.broadcasted_iota(I32, (capacity, tokens), 0).astype(F32)
    picked, scales = [], []
    for e in range(experts):
        one = jnp.where(slot == place[e : e + 1, :], 1.0, 0.0)
        scale = jnp.sum(one * weight[e : e + 1, :], axis=1, keepdims=True)
        picked += [one, one]
        scales += [scale, scale]
    select = jnp.concatenate(picked, axis=0).astype(BF16)
    scale = jnp.concatenate(scales, axis=0)
    select_ref[...] = select
    for copy in copies:
        copy.wait()
    send_ref[:, :LANES] = mm(select, held[0]).astype(BF16)
    send_ref[:, LANES:] = (mm(select, held[1]) * scale).astype(BF16)


def layout_body(core_ref, gate_ref, up_ref, down_ref, gate2_ref, up2_ref, down2_ref, fore_ref, back_ref, rows_ref):
    for i, ref in enumerate((gate_ref, up_ref, gate2_ref, up2_ref)):
        fore_ref[:, i * LANES : (i + 1) * LANES] = ref[...]
    for k in range(back_ref.shape[0] // LANES):
        at = slice(k * LANES, (k + 1) * LANES)
        back_ref[at, :LANES] = down_ref[:, at].astype(F32).T.astype(BF16)
        back_ref[at, LANES:] = down2_ref[:, at].astype(F32).T.astype(BF16)
    for y in range(2 * rows_ref.shape[0]):
        at = pl.ds(pl.multiple_of((2 * y + core_ref[0]) * LANES, LANES), LANES)
        to = slice(y % 2 * LANES, (y % 2 + 1) * LANES)
        for i, ref in enumerate((gate_ref, up_ref, gate2_ref, up2_ref)):
            rows_ref[y // 2, i * LANES : (i + 1) * LANES, to] = ref[at, :].astype(F32).T.astype(BF16)


def expert_body(count, got_ref, fore_ref, back_ref, rows_ref, delta_ref, hidden_ref, chip_ref):
    x = jnp.concatenate([got_ref[t, :, :LANES] for t in range(count)], axis=1)
    pre = mm(x, fore_ref[...])
    d = jnp.concatenate([got_ref[t, :, LANES:] for t in range(count)], axis=1)
    back = mm(d, back_ref[...])
    deltas = []
    for i in range(2):
        gate = pre[:, 2 * i * LANES : (2 * i + 1) * LANES]
        up = pre[:, (2 * i + 1) * LANES : (2 * i + 2) * LANES]
        grad = back[:, i * LANES : (i + 1) * LANES]
        sigma = jax.nn.sigmoid(gate)
        silu = gate * sigma
        if i == 0:
            hidden_ref[...] = (silu * up).astype(BF16)
        deltas.append((grad * up * sigma * (1.0 + gate * (1.0 - sigma))).astype(BF16))
        deltas.append((grad * silu).astype(BF16))
    delta_ref[:, :LANES] = deltas[0]
    delta_ref[:, LANES:] = deltas[1]
    delta = jnp.concatenate(deltas, axis=1)
    for k in range(count // 4):
        part = mm(delta, rows_ref[k]).astype(BF16)
        chip_ref[2 * k] = part[:, :LANES]
        chip_ref[2 * k + 1] = part[:, LANES:]


def weight_body(got_ref, delta_ref, hidden_ref, gate_ref, up_ref, down_ref):
    x = jnp.concatenate([got_ref[0, :, :LANES], got_ref[1, :, :LANES]], axis=1)
    d = jnp.concatenate([got_ref[0, :, LANES:], got_ref[1, :, LANES:]], axis=1)
    grads = mm(x, delta_ref[...], TN)
    gate_ref[...] = grads[:, :LANES].astype(BF16)
    up_ref[...] = grads[:, LANES:].astype(BF16)
    down_ref[...] = mm(hidden_ref[...], d, TN).astype(BF16)


def token_body(at_ref, back_ref, select_ref, cot_ref, grad_ref):
    moe = mm(select_ref[...], back_ref[...], TN).astype(BF16)
    grad_ref[...] = (cot_ref[...].astype(F32) + moe.astype(F32)).astype(BF16)


def part_body(grads_ref, conv_ref, out_ref):
    half = conv_ref.shape[0] // 2
    low = lax.broadcasted_iota(I32, (half, LANES), 1) < LANES // 2
    for k in range(0, grads_ref.shape[0], 2):
        parts = mm(conv_ref[...], jnp.concatenate([grads_ref[k], grads_ref[k + 1]], axis=1))
        for t in range(2):
            top, bottom = (parts[r * half : (r + 1) * half, t * LANES : (t + 1) * LANES] for r in range(2))
            out_ref[2 * k + 2 * t] = jnp.where(low, top, pltpu.roll(bottom, LANES // 2, 1)).astype(BF16)
            out_ref[2 * k + 2 * t + 1] = jnp.where(low, pltpu.roll(top, LANES // 2, 1), bottom).astype(BF16)


def conv_body(grads_ref, weight_ref, sum_ref, outer_ref, outer_grad_ref, scaled_ref):
    total = jnp.zeros(sum_ref.shape, F32)
    for k in range(0, grads_ref.shape[0], 2):
        g = jnp.concatenate([grads_ref[k], grads_ref[k + 1]], axis=1)
        total = total + mm(weight_ref[:, k * LANES : (k + 2) * LANES], g, NT)
    outer_grad_ref[...] = (total * sum_ref[...]).astype(BF16)
    scaled_ref[...] = total * outer_ref[...].astype(F32)


def out_body(tiles_ref, out_ref):
    total = tiles_ref[0].astype(F32)
    for s in range(1, tiles_ref.shape[0]):
        total = total + tiles_ref[s].astype(F32)
    half = LANES // 2
    out_ref[...] = jnp.concatenate([total[:, :half], total[:, half:]], axis=0).T


def per_device(
    cotangent,
    stream,
    routes,
    route_weights,
    gate_weight,
    up_weight,
    down_weight,
    outer_gate,
    inner_gate,
    conv_input,
    conv_taps,
    out_weight,
):
    groups = lax.axis_size("sp")
    ys = lax.axis_size("y")
    tps = 2 * ys
    experts = groups // 2
    tokens, width = stream.shape
    capacity = 3 * tokens // experts
    slots = groups * capacity
    units = gate_weight.shape[2]
    channels = outer_gate.shape[1]
    core = lax.axis_index("c").astype(I32).reshape(1)
    at = (2 * lax.axis_index("y") + lax.axis_index("c")).astype(I32).reshape(1)
    swap = [(0, 1), (1, 0)]

    block = pl.BlockSpec((tokens, LANES), lambda i, at: (0, at[0]))
    whole = lambda *dims: pl.BlockSpec(dims, lambda i, at: (0,) * len(dims))
    send, select = call(
        functools.partial(select_body, experts, capacity),
        (shape((slots, 2 * LANES), BF16), shape((slots, LANES), BF16)),
        (2 * slots * tokens * 2 * LANES, 2**20),
        room=66_000_000,
        in_specs=[pl.BlockSpec(memory_space=pltpu.SMEM)] + [VMEM] * 2 + [pl.BlockSpec(memory_space=pltpu.HBM)] * 2,
        out_specs=[VMEM] * 2,
        scratch_shapes=[pltpu.VMEM((2, tokens, LANES), BF16), pltpu.SemaphoreType.DMA((2,))],
    )(at, routes.T, route_weights.T, stream, cotangent)
    recv = lax.all_to_all(
        send.reshape(groups, capacity, 2 * LANES), "sp", split_axis=0, concat_axis=0, tiled=True
    ).reshape(slots, 2 * LANES)

    outer_t, inner_t, input_t, taps_t = (a.T for a in (outer_gate, inner_gate, conv_input, conv_taps))
    weights = (gate_weight[0], up_weight[0], down_weight[0])
    recv, inner_t, *held = lax.optimization_barrier((recv, inner_t, *weights))
    got = lax.all_gather(recv, TP)
    laid = call(
        layout_body,
        (shape((width, 4 * units), BF16), shape((width, 2 * units), BF16), shape((ys // 2, 4 * units, 2 * LANES), BF16)),
        (2**22, 2**23),
        room=20 * 2**20,
        in_specs=[pl.BlockSpec(memory_space=pltpu.SMEM)] + [VMEM] * 6,
        out_specs=[VMEM] * 3,
    )(core, *held, *(lax.ppermute(a, "c", swap) for a in held))
    outer_f, inner_f, input_f, taps = (a.astype(F32) for a in (outer_t, inner_t, input_t, taps_t))
    mixed = inner_f * input_f
    before = lax.ppermute(mixed[:, -2:], "sp", [(i - 1, i) for i in range(1, groups)])
    padded = jnp.concatenate([before, mixed], axis=1)
    conv_sum = taps[:, 0:1] * padded[:, :-2] + taps[:, 1:2] * padded[:, 1:-1] + taps[:, 2:3] * padded[:, 2:]
    conv_out = (outer_f * conv_sum).astype(BF16)
    got, conv_out, conv_sum, laid = lax.optimization_barrier((got, conv_out, conv_sum, laid))

    rows = 2 * LANES
    fixed = lambda *dims: pl.BlockSpec(dims, lambda i: (0,) * len(dims))
    delta, hidden, chip = call(
        functools.partial(expert_body, tps),
        (shape((slots, 2 * units), BF16), shape((slots, units), BF16), shape((ys, slots, LANES), BF16)),
        (16 * slots * width * units, 2**24),
        room=46 * 2**20,
        grid=(slots // rows,),
        in_specs=[
            pl.BlockSpec((tps, rows, 2 * LANES), lambda i: (0, i, 0)),
            fixed(width, 4 * units),
            fixed(width, 2 * units),
            fixed(ys // 2, 4 * units, 2 * LANES),
        ],
        out_specs=[
            pl.BlockSpec((rows, 2 * units), lambda i: (i, 0)),
            pl.BlockSpec((rows, units), lambda i: (i, 0)),
            pl.BlockSpec((ys, rows, LANES), lambda i: (0, i, 0)),
        ],
    )(got, *laid)
    chip, delta = lax.optimization_barrier((chip, delta))
    half_sums = lax.psum_scatter(chip, "y", scatter_dimension=0)

    gate_grad, up_grad, down_grad = call(
        weight_body,
        (shape((width, units), BF16), shape((width, units), BF16), shape((units, width), BF16)),
        (6 * slots * width * units, 2**24),
        grid=(ys,),
        in_specs=[
            pl.BlockSpec((2, slots, 2 * LANES), lambda i: (i, 0, 0)),
            fixed(slots, 2 * units),
            fixed(slots, units),
        ],
        out_specs=[
            pl.BlockSpec((2 * LANES, units), lambda i: (i, 0)),
            pl.BlockSpec((2 * LANES, units), lambda i: (i, 0)),
            pl.BlockSpec((units, 2 * LANES), lambda i: (0, i)),
        ],
    )(got, delta, hidden)

    half_sums, gate_grad, up_grad, down_grad = lax.optimization_barrier((half_sums, gate_grad, up_grad, down_grad))
    returned = lax.all_to_all(
        half_sums.reshape(groups, capacity, LANES), "sp", split_axis=0, concat_axis=0, tiled=True
    )
    stream_block = call(
        token_body,
        shape((tokens, LANES), BF16),
        (2 * slots * tokens * LANES, 2**21),
        grid_spec=pltpu.PrefetchScalarGridSpec(
            num_scalar_prefetch=1,
            grid=(1,),
            in_specs=[whole(slots, LANES), whole(slots, LANES), block],
            out_specs=whole(tokens, LANES),
        ),
    )(at, returned.reshape(slots, LANES), select, cotangent)
    stream_all = lax.all_gather(stream_block, TP)
    out_parts = call(
        part_body,
        shape((groups, channels // 2, LANES), BF16),
        (2 * tokens * width * channels, 2**20),
        in_specs=[VMEM] * 2,
        out_specs=VMEM,
    )(stream_all, conv_out)
    out_tiles = lax.all_to_all(out_parts, "sp", split_axis=0, concat_axis=0, tiled=True)
    outer_grad, scaled = call(
        conv_body,
        (shape((channels, tokens), BF16), shape((channels, tokens), F32)),
        (2 * tokens * width * channels, 2**20),
        name="conv_grad",
        in_specs=[VMEM] * 4,
        out_specs=[VMEM] * 2,
    )(stream_all, out_weight.T, conv_sum, outer_t)
    out_grad = call(
        out_body,
        shape((channels, width // groups), F32),
        (2**17, 2**19),
        in_specs=[VMEM],
        out_specs=VMEM,
    )(out_tiles)
    later = lax.ppermute(scaled[:, :2], "sp", [(i, i - 1) for i in range(1, groups)])
    extended = jnp.concatenate([scaled, later], axis=1)
    mixed_grad = taps[:, 2:3] * extended[:, :-2] + taps[:, 1:2] * extended[:, 1:-1] + taps[:, 0:1] * extended[:, 2:]
    inner_grad = (mixed_grad * input_f).astype(BF16)
    input_grad = (mixed_grad * inner_f).astype(BF16)
    return (gate_grad[None], up_grad[None], down_grad[None], out_grad, outer_grad.T, inner_grad.T, input_grad.T)


def solution(mesh):
    groups, tps = mesh.devices.shape
    fine = Mesh(mesh.devices.reshape(groups, tps // 2, 2), ("sp", "y", "c"))
    placed = (
        P("sp", None),
        P("sp", None),
        P("sp", None),
        P("sp", None),
        P("sp", None, TP),
        P("sp", None, TP),
        P("sp", TP, None),
        P("sp", TP),
        P("sp", TP),
        P("sp", TP),
        P(None, TP),
        P(None, TP),
    )

    return jax.shard_map(
        per_device,
        mesh=fine,
        in_specs=placed,
        out_specs=(
            P("sp", None, TP),
            P("sp", None, TP),
            P("sp", TP, None),
            P("sp", TP),
            P("sp", TP),
            P("sp", TP),
            P("sp", TP),
        ),
        check_vma=False,
    )
```

```python
import functools

import jax
import jax.numpy as jnp
from jax import lax
from jax.experimental import pallas as pl
from jax.experimental.pallas import tpu as pltpu
from jax.sharding import Mesh, PartitionSpec as P


BF16, F32, I32 = jnp.bfloat16, jnp.float32, jnp.int32
TP = ("y", "c")
NT = (((1,), (1,)), ((), ()))
TN = (((0,), (0,)), ((), ()))
LANES = 128
VMEM = pl.BlockSpec(memory_space=pltpu.VMEM)


def mm(a, b, dims=None):
    if dims is None:
        return jnp.dot(a, b, preferred_element_type=F32)
    return lax.dot_general(a, b, dims, preferred_element_type=F32)


def call(body, out, cost, room=48 * 1024 * 1024, **kw):
    flops, moved = cost
    return pl.pallas_call(
        body,
        out_shape=out,
        cost_estimate=pl.CostEstimate(flops=flops, bytes_accessed=moved, transcendentals=0),
        compiler_params=pltpu.CompilerParams(vmem_limit_bytes=room),
        **kw,
    )


def shape(dims, kind):
    return jax.ShapeDtypeStruct(dims, kind)


def select_body(experts, capacity, at_ref, routes_ref, weights_ref, rows_ref, cot_ref, send_ref, select_ref):
    tokens = routes_ref.shape[1]
    number = lax.broadcasted_iota(I32, (experts, tokens), 0)
    first = routes_ref[0:1, :] == number
    second = routes_ref[1:2, :] == number
    hit = jnp.where(first | second, 1.0, 0.0).astype(F32)
    weight = jnp.where(first, weights_ref[0:1, :], jnp.where(second, weights_ref[1:2, :], 0.0))
    earlier = lax.broadcasted_iota(I32, (tokens, tokens), 0) < lax.broadcasted_iota(I32, (tokens, tokens), 1)
    place = mm(hit.astype(BF16), jnp.where(earlier, 1.0, 0.0).astype(BF16))
    place = jnp.where(hit > 0.0, place, -1.0)
    slot = lax.broadcasted_iota(I32, (capacity, tokens), 0).astype(F32)
    picked, scales = [], []
    for e in range(experts):
        one = jnp.where(slot == place[e : e + 1, :], 1.0, 0.0)
        scale = jnp.sum(one * weight[e : e + 1, :], axis=1, keepdims=True)
        picked += [one, one]
        scales += [scale, scale]
    select = jnp.concatenate(picked, axis=0).astype(BF16)
    scale = jnp.concatenate(scales, axis=0)
    select_ref[...] = select
    send_ref[:, :LANES] = mm(select, rows_ref[...]).astype(BF16)
    send_ref[:, LANES:] = (mm(select, cot_ref[...]) * scale).astype(BF16)


def layout_body(core_ref, gate_ref, up_ref, down_ref, gate2_ref, up2_ref, down2_ref, fore_ref, back_ref, rows_ref):
    for i, ref in enumerate((gate_ref, up_ref, gate2_ref, up2_ref)):
        fore_ref[:, i * LANES : (i + 1) * LANES] = ref[...]
    for k in range(back_ref.shape[0] // LANES):
        at = slice(k * LANES, (k + 1) * LANES)
        back_ref[at, :LANES] = down_ref[:, at].astype(F32).T.astype(BF16)
        back_ref[at, LANES:] = down2_ref[:, at].astype(F32).T.astype(BF16)
    for y in range(2 * rows_ref.shape[0]):
        at = pl.ds(pl.multiple_of((2 * y + core_ref[0]) * LANES, LANES), LANES)
        to = slice(y % 2 * LANES, (y % 2 + 1) * LANES)
        for i, ref in enumerate((gate_ref, up_ref, gate2_ref, up2_ref)):
            rows_ref[y // 2, i * LANES : (i + 1) * LANES, to] = ref[at, :].astype(F32).T.astype(BF16)


def expert_body(count, got_ref, fore_ref, back_ref, rows_ref, delta_ref, hidden_ref, chip_ref):
    x = jnp.concatenate([got_ref[t, :, :LANES] for t in range(count)], axis=1)
    pre = mm(x, fore_ref[...])
    d = jnp.concatenate([got_ref[t, :, LANES:] for t in range(count)], axis=1)
    back = mm(d, back_ref[...])
    deltas = []
    for i in range(2):
        gate = pre[:, 2 * i * LANES : (2 * i + 1) * LANES]
        up = pre[:, (2 * i + 1) * LANES : (2 * i + 2) * LANES]
        grad = back[:, i * LANES : (i + 1) * LANES]
        sigma = jax.nn.sigmoid(gate)
        silu = gate * sigma
        if i == 0:
            hidden_ref[...] = (silu * up).astype(BF16)
        deltas.append((grad * up * sigma * (1.0 + gate * (1.0 - sigma))).astype(BF16))
        deltas.append((grad * silu).astype(BF16))
    delta_ref[:, :LANES] = deltas[0]
    delta_ref[:, LANES:] = deltas[1]
    delta = jnp.concatenate(deltas, axis=1)
    for k in range(count // 4):
        part = mm(delta, rows_ref[k]).astype(BF16)
        chip_ref[2 * k] = part[:, :LANES]
        chip_ref[2 * k + 1] = part[:, LANES:]


def weight_body(got_ref, delta_ref, hidden_ref, gate_ref, up_ref, down_ref):
    x = jnp.concatenate([got_ref[0, :, :LANES], got_ref[1, :, :LANES]], axis=1)
    d = jnp.concatenate([got_ref[0, :, LANES:], got_ref[1, :, LANES:]], axis=1)
    grads = mm(x, delta_ref[...], TN)
    gate_ref[...] = grads[:, :LANES].astype(BF16)
    up_ref[...] = grads[:, LANES:].astype(BF16)
    down_ref[...] = mm(hidden_ref[...], d, TN).astype(BF16)


def token_body(at_ref, back_ref, select_ref, cot_ref, grad_ref):
    moe = mm(select_ref[...], back_ref[...], TN).astype(BF16)
    grad_ref[...] = (cot_ref[...].astype(F32) + moe.astype(F32)).astype(BF16)


def part_body(grads_ref, conv_ref, out_ref):
    half = conv_ref.shape[0] // 2
    low = lax.broadcasted_iota(I32, (half, LANES), 1) < LANES // 2
    for k in range(0, grads_ref.shape[0], 2):
        parts = mm(conv_ref[...], jnp.concatenate([grads_ref[k], grads_ref[k + 1]], axis=1))
        for t in range(2):
            top, bottom = (parts[r * half : (r + 1) * half, t * LANES : (t + 1) * LANES] for r in range(2))
            out_ref[2 * k + 2 * t] = jnp.where(low, top, pltpu.roll(bottom, LANES // 2, 1)).astype(BF16)
            out_ref[2 * k + 2 * t + 1] = jnp.where(low, pltpu.roll(top, LANES // 2, 1), bottom).astype(BF16)


def conv_body(grads_ref, weight_ref, sum_ref, outer_ref, outer_grad_ref, scaled_ref):
    total = jnp.zeros(sum_ref.shape, F32)
    for k in range(0, grads_ref.shape[0], 2):
        g = jnp.concatenate([grads_ref[k], grads_ref[k + 1]], axis=1)
        total = total + mm(weight_ref[:, k * LANES : (k + 2) * LANES], g, NT)
    outer_grad_ref[...] = (total * sum_ref[...]).astype(BF16)
    scaled_ref[...] = total * outer_ref[...].astype(F32)


def out_body(tiles_ref, out_ref):
    total = tiles_ref[0].astype(F32)
    for s in range(1, tiles_ref.shape[0]):
        total = total + tiles_ref[s].astype(F32)
    half = LANES // 2
    out_ref[...] = jnp.concatenate([total[:, :half], total[:, half:]], axis=0).T


def per_device(
    cotangent,
    stream,
    routes,
    route_weights,
    gate_weight,
    up_weight,
    down_weight,
    outer_gate,
    inner_gate,
    conv_input,
    conv_taps,
    out_weight,
):
    groups = lax.axis_size("sp")
    ys = lax.axis_size("y")
    tps = 2 * ys
    experts = groups // 2
    tokens, width = stream.shape
    capacity = 3 * tokens // experts
    slots = groups * capacity
    units = gate_weight.shape[2]
    channels = outer_gate.shape[1]
    core = lax.axis_index("c").astype(I32).reshape(1)
    at = (2 * lax.axis_index("y") + lax.axis_index("c")).astype(I32).reshape(1)
    swap = [(0, 1), (1, 0)]

    block = pl.BlockSpec((tokens, LANES), lambda i, at: (0, at[0]))
    whole = lambda *dims: pl.BlockSpec(dims, lambda i, at: (0,) * len(dims))
    send, select = call(
        functools.partial(select_body, experts, capacity),
        (shape((slots, 2 * LANES), BF16), shape((slots, LANES), BF16)),
        (2 * slots * tokens * 2 * LANES, 2**20),
        room=67_043_328,
        grid_spec=pltpu.PrefetchScalarGridSpec(
            num_scalar_prefetch=1,
            grid=(1,),
            in_specs=[whole(2, tokens), whole(2, tokens), block, block],
            out_specs=[whole(slots, 2 * LANES), whole(slots, LANES)],
        ),
    )(at, routes.T, route_weights.T, stream, cotangent)
    recv = lax.all_to_all(
        send.reshape(groups, capacity, 2 * LANES), "sp", split_axis=0, concat_axis=0, tiled=True
    ).reshape(slots, 2 * LANES)

    outer_t, inner_t, input_t, taps_t = (a.T for a in (outer_gate, inner_gate, conv_input, conv_taps))
    weights = (gate_weight[0], up_weight[0], down_weight[0])
    recv, inner_t, *held = lax.optimization_barrier((recv, inner_t, *weights))
    got = lax.all_gather(recv, TP)
    laid = call(
        layout_body,
        (shape((width, 4 * units), BF16), shape((width, 2 * units), BF16), shape((ys // 2, 4 * units, 2 * LANES), BF16)),
        (2**22, 2**23),
        in_specs=[pl.BlockSpec(memory_space=pltpu.SMEM)] + [VMEM] * 6,
        out_specs=[VMEM] * 3,
    )(core, *held, *(lax.ppermute(a, "c", swap) for a in held))
    outer_f, inner_f, input_f, taps = (a.astype(F32) for a in (outer_t, inner_t, input_t, taps_t))
    mixed = inner_f * input_f
    before = lax.ppermute(mixed[:, -2:], "sp", [(i - 1, i) for i in range(1, groups)])
    padded = jnp.concatenate([before, mixed], axis=1)
    conv_sum = taps[:, 0:1] * padded[:, :-2] + taps[:, 1:2] * padded[:, 1:-1] + taps[:, 2:3] * padded[:, 2:]
    conv_out = (outer_f * conv_sum).astype(BF16)
    got, conv_out, conv_sum, laid = lax.optimization_barrier((got, conv_out, conv_sum, laid))

    rows = 2 * LANES
    fixed = lambda *dims: pl.BlockSpec(dims, lambda i: (0,) * len(dims))
    delta, hidden, chip = call(
        functools.partial(expert_body, tps),
        (shape((slots, 2 * units), BF16), shape((slots, units), BF16), shape((ys, slots, LANES), BF16)),
        (16 * slots * width * units, 2**24),
        grid=(slots // rows,),
        in_specs=[
            pl.BlockSpec((tps, rows, 2 * LANES), lambda i: (0, i, 0)),
            fixed(width, 4 * units),
            fixed(width, 2 * units),
            fixed(ys // 2, 4 * units, 2 * LANES),
        ],
        out_specs=[
            pl.BlockSpec((rows, 2 * units), lambda i: (i, 0)),
            pl.BlockSpec((rows, units), lambda i: (i, 0)),
            pl.BlockSpec((ys, rows, LANES), lambda i: (0, i, 0)),
        ],
    )(got, *laid)
    chip, delta = lax.optimization_barrier((chip, delta))
    half_sums = lax.psum_scatter(chip, "y", scatter_dimension=0)

    gate_grad, up_grad, down_grad = call(
        weight_body,
        (shape((width, units), BF16), shape((width, units), BF16), shape((units, width), BF16)),
        (6 * slots * width * units, 2**24),
        grid=(ys,),
        in_specs=[
            pl.BlockSpec((2, slots, 2 * LANES), lambda i: (i, 0, 0)),
            fixed(slots, 2 * units),
            fixed(slots, units),
        ],
        out_specs=[
            pl.BlockSpec((2 * LANES, units), lambda i: (i, 0)),
            pl.BlockSpec((2 * LANES, units), lambda i: (i, 0)),
            pl.BlockSpec((units, 2 * LANES), lambda i: (0, i)),
        ],
    )(got, delta, hidden)

    half_sums, gate_grad, up_grad, down_grad = lax.optimization_barrier((half_sums, gate_grad, up_grad, down_grad))
    returned = lax.all_to_all(
        half_sums.reshape(groups, capacity, LANES), "sp", split_axis=0, concat_axis=0, tiled=True
    )
    stream_block = call(
        token_body,
        shape((tokens, LANES), BF16),
        (2 * slots * tokens * LANES, 2**21),
        grid_spec=pltpu.PrefetchScalarGridSpec(
            num_scalar_prefetch=1,
            grid=(1,),
            in_specs=[whole(slots, LANES), whole(slots, LANES), block],
            out_specs=whole(tokens, LANES),
        ),
    )(at, returned.reshape(slots, LANES), select, cotangent)
    stream_all = lax.all_gather(stream_block, TP)
    out_parts = call(
        part_body,
        shape((groups, channels // 2, LANES), BF16),
        (2 * tokens * width * channels, 2**20),
        in_specs=[VMEM] * 2,
        out_specs=VMEM,
    )(stream_all, conv_out)
    out_tiles = lax.all_to_all(out_parts, "sp", split_axis=0, concat_axis=0, tiled=True)
    outer_grad, scaled = call(
        conv_body,
        (shape((channels, tokens), BF16), shape((channels, tokens), F32)),
        (2 * tokens * width * channels, 2**20),
        name="conv_grad",
        in_specs=[VMEM] * 4,
        out_specs=[VMEM] * 2,
    )(stream_all, out_weight.T, conv_sum, outer_t)
    out_grad = call(
        out_body,
        shape((channels, width // groups), F32),
        (2**17, 2**19),
        in_specs=[VMEM],
        out_specs=VMEM,
    )(out_tiles)
    later = lax.ppermute(scaled[:, :2], "sp", [(i, i - 1) for i in range(1, groups)])
    extended = jnp.concatenate([scaled, later], axis=1)
    mixed_grad = taps[:, 2:3] * extended[:, :-2] + taps[:, 1:2] * extended[:, 1:-1] + taps[:, 0:1] * extended[:, 2:]
    inner_grad = (mixed_grad * input_f).astype(BF16)
    input_grad = (mixed_grad * inner_f).astype(BF16)
    return (gate_grad[None], up_grad[None], down_grad[None], out_grad, outer_grad.T, inner_grad.T, input_grad.T)


def solution(mesh):
    groups, tps = mesh.devices.shape
    fine = Mesh(mesh.devices.reshape(groups, tps // 2, 2), ("sp", "y", "c"))
    placed = (
        P("sp", None),
        P("sp", None),
        P("sp", None),
        P("sp", None),
        P("sp", None, TP),
        P("sp", None, TP),
        P("sp", TP, None),
        P("sp", TP),
        P("sp", TP),
        P("sp", TP),
        P(None, TP),
        P(None, TP),
    )

    return jax.shard_map(
        per_device,
        mesh=fine,
        in_specs=placed,
        out_specs=(
            P("sp", None, TP),
            P("sp", None, TP),
            P("sp", TP, None),
            P("sp", TP),
            P("sp", TP),
            P("sp", TP),
            P("sp", TP),
        ),
        check_vma=False,
    )
```

```python
import functools

import jax
import jax.numpy as jnp
from jax import lax
from jax.experimental import pallas as pl
from jax.experimental.pallas import tpu as pltpu
from jax.sharding import Mesh, PartitionSpec as P


BF16, F32, I32 = jnp.bfloat16, jnp.float32, jnp.int32
TP = ("y", "c")
NT = (((1,), (1,)), ((), ()))
TN = (((0,), (0,)), ((), ()))
LANES = 128
VMEM = pl.BlockSpec(memory_space=pltpu.VMEM)


def mm(a, b, dims=None):
    if dims is None:
        return jnp.dot(a, b, preferred_element_type=F32)
    return lax.dot_general(a, b, dims, preferred_element_type=F32)


def call(body, out, cost, room=48 * 1024 * 1024, **kw):
    flops, moved = cost
    return pl.pallas_call(
        body,
        out_shape=out,
        cost_estimate=pl.CostEstimate(flops=flops, bytes_accessed=moved, transcendentals=0),
        compiler_params=pltpu.CompilerParams(vmem_limit_bytes=room),
        **kw,
    )


def shape(dims, kind):
    return jax.ShapeDtypeStruct(dims, kind)


def select_body(experts, capacity, at_ref, routes_ref, weights_ref, rows_ref, cot_ref, send_ref, select_ref):
    tokens = routes_ref.shape[1]
    number = lax.broadcasted_iota(I32, (experts, tokens), 0)
    first = routes_ref[0:1, :] == number
    second = routes_ref[1:2, :] == number
    hit = jnp.where(first | second, 1.0, 0.0).astype(F32)
    weight = jnp.where(first, weights_ref[0:1, :], jnp.where(second, weights_ref[1:2, :], 0.0))
    earlier = lax.broadcasted_iota(I32, (tokens, tokens), 0) < lax.broadcasted_iota(I32, (tokens, tokens), 1)
    place = mm(hit.astype(BF16), jnp.where(earlier, 1.0, 0.0).astype(BF16))
    place = jnp.where(hit > 0.0, place, -1.0)
    slot = lax.broadcasted_iota(I32, (capacity, tokens), 0).astype(F32)
    picked, scales = [], []
    for e in range(experts):
        one = jnp.where(slot == place[e : e + 1, :], 1.0, 0.0)
        scale = jnp.sum(one * weight[e : e + 1, :], axis=1, keepdims=True)
        picked += [one, one]
        scales += [scale, scale]
    select = jnp.concatenate(picked, axis=0).astype(BF16)
    scale = jnp.concatenate(scales, axis=0)
    select_ref[...] = select
    send_ref[:, :LANES] = mm(select, rows_ref[...]).astype(BF16)
    send_ref[:, LANES:] = (mm(select, cot_ref[...]) * scale).astype(BF16)


def layout_body(core_ref, gate_ref, up_ref, down_ref, gate2_ref, up2_ref, down2_ref, fore_ref, back_ref, rows_ref):
    for i, ref in enumerate((gate_ref, up_ref, gate2_ref, up2_ref)):
        fore_ref[:, i * LANES : (i + 1) * LANES] = ref[...]
    for k in range(back_ref.shape[0] // LANES):
        at = slice(k * LANES, (k + 1) * LANES)
        back_ref[at, :LANES] = down_ref[:, at].astype(F32).T.astype(BF16)
        back_ref[at, LANES:] = down2_ref[:, at].astype(F32).T.astype(BF16)
    for y in range(2 * rows_ref.shape[0]):
        at = pl.ds(pl.multiple_of((2 * y + core_ref[0]) * LANES, LANES), LANES)
        to = slice(y % 2 * LANES, (y % 2 + 1) * LANES)
        for i, ref in enumerate((gate_ref, up_ref, gate2_ref, up2_ref)):
            rows_ref[y // 2, i * LANES : (i + 1) * LANES, to] = ref[at, :].astype(F32).T.astype(BF16)


def expert_body(count, got_ref, fore_ref, back_ref, rows_ref, delta_ref, hidden_ref, chip_ref):
    x = jnp.concatenate([got_ref[t, :, :LANES] for t in range(count)], axis=1)
    pre = mm(x, fore_ref[...])
    d = jnp.concatenate([got_ref[t, :, LANES:] for t in range(count)], axis=1)
    back = mm(d, back_ref[...])
    deltas = []
    for i in range(2):
        gate = pre[:, 2 * i * LANES : (2 * i + 1) * LANES]
        up = pre[:, (2 * i + 1) * LANES : (2 * i + 2) * LANES]
        grad = back[:, i * LANES : (i + 1) * LANES]
        sigma = jax.nn.sigmoid(gate)
        silu = gate * sigma
        if i == 0:
            hidden_ref[...] = (silu * up).astype(BF16)
        deltas.append((grad * up * sigma * (1.0 + gate * (1.0 - sigma))).astype(BF16))
        deltas.append((grad * silu).astype(BF16))
    delta_ref[:, :LANES] = deltas[0]
    delta_ref[:, LANES:] = deltas[1]
    delta = jnp.concatenate(deltas, axis=1)
    for k in range(count // 4):
        part = mm(delta, rows_ref[k]).astype(BF16)
        chip_ref[2 * k] = part[:, :LANES]
        chip_ref[2 * k + 1] = part[:, LANES:]


def weight_body(got_ref, delta_ref, hidden_ref, gate_ref, up_ref, down_ref):
    x = jnp.concatenate([got_ref[0, :, :LANES], got_ref[1, :, :LANES]], axis=1)
    d = jnp.concatenate([got_ref[0, :, LANES:], got_ref[1, :, LANES:]], axis=1)
    grads = mm(x, delta_ref[...], TN)
    gate_ref[...] = grads[:, :LANES].astype(BF16)
    up_ref[...] = grads[:, LANES:].astype(BF16)
    down_ref[...] = mm(hidden_ref[...], d, TN).astype(BF16)


def token_body(at_ref, back_ref, select_ref, cot_ref, grad_ref):
    moe = mm(select_ref[...], back_ref[...], TN).astype(BF16)
    grad_ref[...] = (cot_ref[...].astype(F32) + moe.astype(F32)).astype(BF16)


def part_body(grads_ref, conv_ref, out_ref):
    half = conv_ref.shape[0] // 2
    low = lax.broadcasted_iota(I32, (half, LANES), 1) < LANES // 2
    for k in range(0, grads_ref.shape[0], 2):
        parts = mm(conv_ref[...], jnp.concatenate([grads_ref[k], grads_ref[k + 1]], axis=1))
        for t in range(2):
            top, bottom = (parts[r * half : (r + 1) * half, t * LANES : (t + 1) * LANES] for r in range(2))
            out_ref[2 * k + 2 * t] = jnp.where(low, top, pltpu.roll(bottom, LANES // 2, 1)).astype(BF16)
            out_ref[2 * k + 2 * t + 1] = jnp.where(low, pltpu.roll(top, LANES // 2, 1), bottom).astype(BF16)


def conv_body(grads_ref, weight_ref, sum_ref, outer_ref, outer_grad_ref, scaled_ref):
    total = jnp.zeros(sum_ref.shape, F32)
    for k in range(0, grads_ref.shape[0], 2):
        g = jnp.concatenate([grads_ref[k], grads_ref[k + 1]], axis=1)
        total = total + mm(weight_ref[:, k * LANES : (k + 2) * LANES], g, NT)
    outer_grad_ref[...] = (total * sum_ref[...]).astype(BF16)
    scaled_ref[...] = total * outer_ref[...].astype(F32)


def out_body(tiles_ref, out_ref):
    total = tiles_ref[0].astype(F32)
    for s in range(1, tiles_ref.shape[0]):
        total = total + tiles_ref[s].astype(F32)
    half = LANES // 2
    out_ref[...] = jnp.concatenate([total[:, :half], total[:, half:]], axis=0).T


def per_device(
    cotangent,
    stream,
    routes,
    route_weights,
    gate_weight,
    up_weight,
    down_weight,
    outer_gate,
    inner_gate,
    conv_input,
    conv_taps,
    out_weight,
):
    groups = lax.axis_size("sp")
    ys = lax.axis_size("y")
    tps = 2 * ys
    experts = groups // 2
    tokens, width = stream.shape
    capacity = 3 * tokens // experts
    slots = groups * capacity
    units = gate_weight.shape[2]
    channels = outer_gate.shape[1]
    core = lax.axis_index("c").astype(I32).reshape(1)
    at = (2 * lax.axis_index("y") + lax.axis_index("c")).astype(I32).reshape(1)
    swap = [(0, 1), (1, 0)]

    block = pl.BlockSpec((tokens, LANES), lambda i, at: (0, at[0]))
    whole = lambda *dims: pl.BlockSpec(dims, lambda i, at: (0,) * len(dims))
    send, select = call(
        functools.partial(select_body, experts, capacity),
        (pltpu.VMEM((slots, 2 * LANES), BF16), pltpu.VMEM((slots, LANES), BF16)),
        (2 * slots * tokens * 2 * LANES, 2**20),
        room=60_000_000,
        grid_spec=pltpu.PrefetchScalarGridSpec(
            num_scalar_prefetch=1,
            grid=(1,),
            in_specs=[whole(2, tokens), whole(2, tokens), block, block],
            out_specs=[whole(slots, 2 * LANES), whole(slots, LANES)],
        ),
    )(at, routes.T, route_weights.T, stream, cotangent)
    recv = lax.all_to_all(
        send.reshape(groups, capacity, 2 * LANES), "sp", split_axis=0, concat_axis=0, tiled=True
    ).reshape(slots, 2 * LANES)

    outer_t, inner_t, input_t, taps_t = (a.T for a in (outer_gate, inner_gate, conv_input, conv_taps))
    weights = (gate_weight[0], up_weight[0], down_weight[0])
    recv, inner_t, *held = lax.optimization_barrier((recv, inner_t, *weights))
    got = lax.all_gather(recv, TP)
    laid = call(
        layout_body,
        (pltpu.HBM((width, 4 * units), BF16), pltpu.HBM((width, 2 * units), BF16), pltpu.HBM((ys // 2, 4 * units, 2 * LANES), BF16)),
        (2**22, 2**23),
        in_specs=[pl.BlockSpec(memory_space=pltpu.SMEM)] + [VMEM] * 6,
        out_specs=[VMEM] * 3,
    )(core, *held, *(lax.ppermute(a, "c", swap) for a in held))
    outer_f, inner_f, input_f, taps = (a.astype(F32) for a in (outer_t, inner_t, input_t, taps_t))
    mixed = inner_f * input_f
    before = lax.ppermute(mixed[:, -2:], "sp", [(i - 1, i) for i in range(1, groups)])
    padded = jnp.concatenate([before, mixed], axis=1)
    conv_sum = taps[:, 0:1] * padded[:, :-2] + taps[:, 1:2] * padded[:, 1:-1] + taps[:, 2:3] * padded[:, 2:]
    conv_out = (outer_f * conv_sum).astype(BF16)
    got, conv_out, conv_sum, laid = lax.optimization_barrier((got, conv_out, conv_sum, laid))

    rows = 2 * LANES
    fixed = lambda *dims: pl.BlockSpec(dims, lambda i: (0,) * len(dims))
    delta, hidden, chip = call(
        functools.partial(expert_body, tps),
        (shape((slots, 2 * units), BF16), shape((slots, units), BF16), shape((ys, slots, LANES), BF16)),
        (16 * slots * width * units, 2**24),
        room=56 * 2**20,
        grid=(slots // rows,),
        in_specs=[
            pl.BlockSpec((tps, rows, 2 * LANES), lambda i: (0, i, 0)),
            fixed(width, 4 * units),
            fixed(width, 2 * units),
            fixed(ys // 2, 4 * units, 2 * LANES),
        ],
        out_specs=[
            pl.BlockSpec((rows, 2 * units), lambda i: (i, 0)),
            pl.BlockSpec((rows, units), lambda i: (i, 0)),
            pl.BlockSpec((ys, rows, LANES), lambda i: (0, i, 0)),
        ],
    )(got, *laid)
    chip, delta = lax.optimization_barrier((chip, delta))
    half_sums = lax.psum_scatter(chip, "y", scatter_dimension=0)

    gate_grad, up_grad, down_grad = call(
        weight_body,
        (shape((width, units), BF16), shape((width, units), BF16), shape((units, width), BF16)),
        (6 * slots * width * units, 2**24),
        grid=(ys,),
        in_specs=[
            pl.BlockSpec((2, slots, 2 * LANES), lambda i: (i, 0, 0)),
            fixed(slots, 2 * units),
            fixed(slots, units),
        ],
        out_specs=[
            pl.BlockSpec((2 * LANES, units), lambda i: (i, 0)),
            pl.BlockSpec((2 * LANES, units), lambda i: (i, 0)),
            pl.BlockSpec((units, 2 * LANES), lambda i: (0, i)),
        ],
    )(got, delta, hidden)

    half_sums, gate_grad, up_grad, down_grad = lax.optimization_barrier((half_sums, gate_grad, up_grad, down_grad))
    returned = lax.all_to_all(
        half_sums.reshape(groups, capacity, LANES), "sp", split_axis=0, concat_axis=0, tiled=True
    )
    stream_block = call(
        token_body,
        shape((tokens, LANES), BF16),
        (2 * slots * tokens * LANES, 2**21),
        grid_spec=pltpu.PrefetchScalarGridSpec(
            num_scalar_prefetch=1,
            grid=(1,),
            in_specs=[whole(slots, LANES), whole(slots, LANES), block],
            out_specs=whole(tokens, LANES),
        ),
    )(at, returned.reshape(slots, LANES), select, cotangent)
    stream_all = lax.all_gather(stream_block, TP)
    out_parts = call(
        part_body,
        shape((groups, channels // 2, LANES), BF16),
        (2 * tokens * width * channels, 2**20),
        in_specs=[VMEM] * 2,
        out_specs=VMEM,
    )(stream_all, conv_out)
    out_tiles = lax.all_to_all(out_parts, "sp", split_axis=0, concat_axis=0, tiled=True)
    outer_grad, scaled = call(
        conv_body,
        (shape((channels, tokens), BF16), shape((channels, tokens), F32)),
        (2 * tokens * width * channels, 2**20),
        name="conv_grad",
        in_specs=[VMEM] * 4,
        out_specs=[VMEM] * 2,
    )(stream_all, out_weight.T, conv_sum, outer_t)
    out_grad = call(
        out_body,
        shape((channels, width // groups), F32),
        (2**17, 2**19),
        in_specs=[VMEM],
        out_specs=VMEM,
    )(out_tiles)
    later = lax.ppermute(scaled[:, :2], "sp", [(i, i - 1) for i in range(1, groups)])
    extended = jnp.concatenate([scaled, later], axis=1)
    mixed_grad = taps[:, 2:3] * extended[:, :-2] + taps[:, 1:2] * extended[:, 1:-1] + taps[:, 0:1] * extended[:, 2:]
    inner_grad = (mixed_grad * input_f).astype(BF16)
    input_grad = (mixed_grad * inner_f).astype(BF16)
    return (gate_grad[None], up_grad[None], down_grad[None], out_grad, outer_grad.T, inner_grad.T, input_grad.T)


def solution(mesh):
    groups, tps = mesh.devices.shape
    fine = Mesh(mesh.devices.reshape(groups, tps // 2, 2), ("sp", "y", "c"))
    placed = (
        P("sp", None),
        P("sp", None),
        P("sp", None),
        P("sp", None),
        P("sp", None, TP),
        P("sp", None, TP),
        P("sp", TP, None),
        P("sp", TP),
        P("sp", TP),
        P("sp", TP),
        P(None, TP),
        P(None, TP),
    )

    return jax.shard_map(
        per_device,
        mesh=fine,
        in_specs=placed,
        out_specs=(
            P("sp", None, TP),
            P("sp", None, TP),
            P("sp", TP, None),
            P("sp", TP),
            P("sp", TP),
            P("sp", TP),
            P("sp", TP),
        ),
        check_vma=False,
    )
```
